512 devices in a mesh: sp: 32 (over z, core), tp: 16 (over y, x).
Axes of the slice: x: 4, y: 4, z: 16, core: 2. Of those that a mesh axis runs over, the one named last changes fastest.
Arguments:
- moe_input: bfloat16 [4096, 2048], P('sp', 'tp'), may hold values from -6 to 6
- cotangent: bfloat16 [4096, 2048], P('sp', 'tp'), may hold values from -6 to 6
- routes: int32 [4096, 2], P('sp'), may hold values from 0 to 31, all different within a row; in each aligned block of 128 rows (0 to 127, 128 to 255, ...) at most 10 rows name the same one
- route_weights: float32 [4096, 2], P('sp'), may hold values from 0.2 to 1
- gate_branch: bfloat16 [4096, 2560], P('sp', 'tp'), may hold values from -6 to 6
- log_decay: float32 [4096, 2560], P('sp', 'tp'), may hold values from -0.12 to 0
- states: float32 [4096, 2560], P('sp', 'tp'), may hold values from -6 to 6
- w_gate: bfloat16 [32, 2048, 2048], P('sp', None, 'tp'), may hold values from -0.125 to 0.125
- w_up: bfloat16 [32, 2048, 2048], P('sp', None, 'tp'), may hold values from -0.125 to 0.125
- w_down: bfloat16 [32, 2048, 2048], P('sp', 'tp'), may hold values from -0.125 to 0.125
- out_proj: bfloat16 [2048, 2560], P('sp', 'tp'), may hold values from -0.125 to 0.125
Outputs:
- grad_w_gate: float32 [32, 2048, 2048], P('sp', None, 'tp')
- grad_w_up: float32 [32, 2048, 2048], P('sp', None, 'tp')
- grad_w_down: float32 [32, 2048, 2048], P('sp', 'tp')
- grad_out_proj: float32 [2048, 2560], P('sp', 'tp')
- grad_gate_branch: bfloat16 [4096, 2560], P('sp', 'tp')
- grad_log_decay: bfloat16 [4096, 2560], P('sp', 'tp')
- grad_input_term: float32 [4096, 2560], P('sp', 'tp')
The draws below stay inside these ranges and needn't reach their ends.
Inputs may be any that keep to these rules, and one draw needn't show every extreme that they name: `routes`: in the rows of one device no expert is named by more than 10 entries, and in every draw some expert is named by exactly 10 entries of one device's rows.
All inputs are finite; a program needn't handle non-finite values.
Results may differ from the reference program's by a relative error of at most 0.025.
Values may be sent and summed in bfloat16 or wider, within the bound.
A program may use at most 64 MiB of HBM per device.

```python
import math
import jax
import jax.numpy as jnp
import numpy as np
from jax import lax

D = 2048
W = 2560
F = 2048
TOP = 2
TOK_DEV = 128
EXPERTS = 32
TOKENS = 4096
CAP = 10
N_SP = 32
N_TP = 16


def draw_log_decay(key, part):
    key_kind, key_rate, key_block, key_cell = jax.random.split(key, 4)
    slow_share = 50
    slow_mask = jax.random.randint(key_kind, (W,), 0, 100) < slow_share
    slow_rate = jax.random.uniform(key_rate, (W,), jnp.float32, 0.3, 0.5) * math.log(10.0) / TOKENS
    fast_rate = jax.random.uniform(jax.random.fold_in(key_rate, 7), (W,), jnp.float32, 1.0 / 60.0, 1.0 / 25.0)
    chan_rates = jnp.where(slow_mask, slow_rate, fast_rate)
    block_scale = jnp.exp(jax.random.uniform(key_block, (TOKENS // TOK_DEV, W), jnp.float32, -math.log(2.0), math.log(2.0)))
    block_scale = jnp.repeat(block_scale, TOK_DEV, axis=0)
    cell_scale = jax.random.uniform(key_cell, (TOKENS, W), jnp.float32, 0.5, 1.5)
    return -(chan_rates[None, :] * block_scale * cell_scale)


def strengthened(entries, rng, source, target, blocks, factor):
    owner, partner = [(jnp.arange(entries.shape[position]) // (entries.shape[position] // blocks)).reshape([-1 if axis == position else 1 for axis in range(entries.ndim)]) for position in (source, target)]
    chosen = jax.random.permutation(rng, blocks)[partner]
    strong = (owner == chosen) | (owner == (partner + blocks // 2) % blocks)
    return jnp.where(strong, factor * entries, entries)


def shard_levels(key, dims, cuts, smallest, largest):
    loudness, own = 1.0, jax.random.fold_in(key, 6)
    for dim, blocks in cuts:
        heights = jnp.exp(jax.random.uniform(jax.random.fold_in(own, dim), (blocks,), jnp.float32, smallest / len(cuts), largest / len(cuts)))
        loudness = loudness * jnp.repeat(heights, dims[dim] // blocks).reshape([-1 if axis == dim else 1 for axis in range(len(dims))])
    return loudness


def deal_out(own_key, own, number, rows, count, top, bound, lean):
    ranking = jax.random.permutation(own_key, count)
    heavy_load, ordinary = load_shares(count, rows * top, bound, lean, True), load_shares(count, rows * top, bound, lean, False)
    places = jnp.arange(count)

    def named(lengths, turn):
        used = int((lengths > 0).sum())
        fixed = max(1, used // 4)
        moved = fixed + (places - fixed + turn * (used - fixed)) % max(1, count - fixed)
        return jnp.zeros((count,), jnp.int32).at[ranking[jnp.where(places < fixed, places, moved)]].set(jnp.asarray(lengths, jnp.int32))

    lengths = jnp.where(number % 4 == 0, named(heavy_load, number // 4), named(ordinary, number - number // 4 - 1))
    mixed = jax.random.permutation(jax.random.fold_in(own, 3), count)
    source_of, taker = mixed[0:count // 2 * 2:2], mixed[1:count // 2 * 2:2]
    slack = jnp.minimum(lengths[source_of] - 1, bound - lengths[taker]) // 2
    slack = jnp.where((source_of == ranking[0]) | (taker == ranking[0]) | (lengths[taker] == 0), 0, jnp.maximum(slack, 0))
    moved = jax.random.randint(jax.random.fold_in(own, 4), (count // 2,), 0, 1 << 20) % (slack + 1)
    lengths = lengths.at[source_of].add(-moved).at[taker].add(moved)
    items = jnp.searchsorted(jnp.cumsum(lengths), jnp.arange(rows * top), side="right").astype(jnp.int32)
    listing = items.reshape(top, rows).T
    listing = listing[jax.random.permutation(jax.random.fold_in(own, 1), rows)]
    turn = jax.random.randint(jax.random.fold_in(own, 2), (rows, 1), 0, top)
    return jnp.take_along_axis(listing, (jnp.arange(top)[None, :] + turn) % top, axis=1)


def load_shares(amount, total, limit, skew, full):
    weights = [(1 << 20) // math.isqrt(standing ** skew) + 1 for standing in range(1, amount + 1)]
    largest = limit if full else min(limit, max(-(-total // amount), total * weights[0] // sum(weights)))
    least = 1 if total - largest >= amount - 1 else 0
    counts, spare = [largest] + [least] * (amount - 1), total - largest - least * (amount - 1)
    while spare > 0:
        free = [i for i in range(1, amount) if counts[i] < largest] or [i for i in range(1, amount) if counts[i] < limit]
        whole, budget = sum([weights[i] for i in free]), spare
        for i in free:
            extra = min(limit - counts[i], max(1, budget * weights[i] // whole), spare)
            counts[i] = counts[i] + extra
            spare = spare - extra
    return np.array(counts)


def gaussian(stream_key, shape, width, bound, cuts=(), kind=jnp.bfloat16):
    result = width * jax.random.normal(stream_key, shape, jnp.float32)
    if cuts:
        result = result * shard_levels(stream_key, shape, cuts, -0.22, 0.18)
    return jnp.clip(result, -bound, bound).astype(kind)


def noise_with(key, shape, deviation, reach, cuts, heavy, kind=jnp.bfloat16):
    result = deviation * jax.random.normal(key, shape, jnp.float32)
    if cuts:
        result = result * shard_levels(key, shape, cuts, -0.22, 0.18)
    return jnp.clip(strengthened(result, jax.random.fold_in(key, 3), *heavy), -reach, reach).astype(kind)


def setup_inputs(seed: int = 0) -> dict:
    key_list = jax.random.split(jax.random.key(seed), 12)
    moe_input = gaussian(key_list[0], (TOKENS, D), 1.0, 6.0, ((0, 32), (1, 16)))
    cotangent = noise_with(key_list[1], (TOKENS, D), 1.0, 6.0, ((0, 32), (1, 16)), (0, 1, 32, 2.75))
    routes_keys = jax.random.split(jax.random.fold_in(key_list[2], 1), TOKENS // TOK_DEV)
    routes_turns = jax.random.permutation(jax.random.fold_in(key_list[2], 3), TOKENS // TOK_DEV)
    routes = jax.vmap(lambda own, number: deal_out(jax.random.fold_in(key_list[2], 2), own, number, TOK_DEV, EXPERTS, TOP, CAP, 2))(routes_keys, routes_turns).reshape((TOKENS, TOP))
    route_weights = jnp.clip(0.2 + 0.8 * jax.random.uniform(key_list[3], (TOKENS, TOP), jnp.float32) ** shard_levels(key_list[3], (TOKENS, TOP), ((0, 32),), -0.2, 0.2), 0.2, 1.0)
    gate_branch = gaussian(key_list[4], (TOKENS, W), 1.0, 6.0, ((0, 32), (1, 16)))
    log_decay = draw_log_decay(jax.random.fold_in(key_list[11], 71), 0)
    states = gaussian(key_list[6], (TOKENS, W), 1.0, 6.0, ((0, 32), (1, 16)), jnp.float32)
    w_gate = gaussian(key_list[7], (EXPERTS, D, F), D ** -0.5, 0.125, ((0, 32), (2, 16)))
    w_up = gaussian(key_list[8], (EXPERTS, D, F), D ** -0.5, 0.125, ((0, 32), (2, 16)))
    w_down = gaussian(key_list[9], (EXPERTS, F, D), F ** -0.5, 0.125, ((0, 32), (1, 16)))
    out_proj = gaussian(key_list[10], (D, W), W ** -0.5, 0.125, ((0, 32), (1, 16)))
    return dict(moe_input=moe_input, cotangent=cotangent, routes=routes, route_weights=route_weights, gate_branch=gate_branch, log_decay=log_decay, states=states, w_gate=w_gate, w_up=w_up, w_down=w_down, out_proj=out_proj)


def silu_parts(pre_gate):
    sigmoid_val = jax.nn.sigmoid(pre_gate)
    return (pre_gate * sigmoid_val, sigmoid_val * (1.0 + pre_gate * (1.0 - sigmoid_val)))

def combine_pair(left_pair, right_pair):
    return (left_pair[0] * right_pair[0], right_pair[0] * left_pair[1] + right_pair[1])

def expert_backward(row_data, scaled, gate_w, up_w, down_w):
    pre_gate = jnp.dot(row_data, gate_w, preferred_element_type=jnp.float32)
    pre_up = jnp.dot(row_data, up_w, preferred_element_type=jnp.float32)
    active, slope = silu_parts(pre_gate)
    hidden = (active * pre_up).astype(jnp.bfloat16)
    grad_down = jnp.dot(hidden.T, scaled, preferred_element_type=jnp.float32)
    grad_hidden = jnp.dot(scaled, down_w.T, preferred_element_type=jnp.float32)
    grad_pre_gate = (grad_hidden * pre_up * slope).astype(jnp.bfloat16)
    grad_pre_up = (grad_hidden * active).astype(jnp.bfloat16)
    grad_gate_w = jnp.dot(row_data.T, grad_pre_gate, preferred_element_type=jnp.float32)
    grad_up_w = jnp.dot(row_data.T, grad_pre_up, preferred_element_type=jnp.float32)
    row_total = grad_pre_gate.shape[0]
    blocked_gate = grad_pre_gate.reshape(row_total, N_TP, F // N_TP).astype(jnp.float32)
    blocked_up = grad_pre_up.reshape(row_total, N_TP, F // N_TP).astype(jnp.float32)
    weight_gate = gate_w.reshape(D, N_TP, F // N_TP).astype(jnp.float32)
    weight_up = up_w.reshape(D, N_TP, F // N_TP).astype(jnp.float32)
    block_terms = jnp.einsum('nbf,dbf->bnd', blocked_gate, weight_gate) + jnp.einsum('nbf,dbf->bnd', blocked_up, weight_up)
    rounded = lax.optimization_barrier(block_terms.astype(jnp.bfloat16))
    entry_grad = lax.optimization_barrier(jnp.sum(rounded.astype(jnp.float32), axis=0)).astype(jnp.bfloat16)
    return (grad_gate_w, grad_up_w, grad_down, entry_grad)

def reference(moe_input, cotangent, routes, route_weights, gate_branch, log_decay, states, w_gate, w_up, w_down, out_proj):
    flat_routes = routes.reshape(-1).astype(jnp.int32)
    flat_weights = route_weights.reshape(-1)
    owners = jnp.arange(TOKENS * TOP, dtype=jnp.int32) // TOP
    room = N_SP * CAP

    def per_expert(totals, inputs):
        expert, gate_w, up_w, down_w = inputs
        sorted_idx = jnp.argsort((flat_routes != expert).astype(jnp.int32), stable=True)[:room].astype(jnp.int32)
        live_rows = (flat_routes[sorted_idx] == expert).astype(jnp.float32)
        token_idx = owners[sorted_idx]
        row_data = moe_input[token_idx]
        scaled = ((live_rows * flat_weights[sorted_idx])[:, None] * cotangent[token_idx].astype(jnp.float32)).astype(jnp.bfloat16)
        grad_gate_w, grad_up_w, grad_down, entry_grad = expert_backward(row_data, scaled, gate_w, up_w, down_w)
        totals = totals.at[token_idx].add(entry_grad.astype(jnp.float32) * live_rows[:, None])
        return (totals, (grad_gate_w, grad_up_w, grad_down))
    totals, grads = lax.scan(per_expert, jnp.zeros((TOKENS, D), jnp.float32), (jnp.arange(EXPERTS, dtype=jnp.int32), w_gate, w_up, w_down))
    grad_w_gate, grad_w_up, grad_w_down = grads
    grad_tokens = (cotangent.astype(jnp.float32) + totals).astype(jnp.bfloat16)
    active_gate, pullback = jax.vjp(jax.nn.gelu, gate_branch.astype(jnp.float32))
    mixed_in = (active_gate * states).astype(jnp.bfloat16)
    grad_out_proj = jnp.dot(grad_tokens.T, mixed_in, preferred_element_type=jnp.float32)
    grad_mixed = jnp.dot(grad_tokens, out_proj, preferred_element_type=jnp.float32)
    grad_gate_branch = pullback(grad_mixed * states)[0].astype(jnp.bfloat16)
    grad_state = grad_mixed * active_gate
    decays = jnp.exp(log_decay)
    next_decay = jnp.concatenate([decays[1:], jnp.zeros_like(decays[:1])], axis=0)
    _, back_flip = lax.associative_scan(combine_pair, (jnp.flip(next_decay, 0), jnp.flip(grad_state, 0)))
    grad_input_term = jnp.flip(back_flip, 0)
    prev_states = jnp.concatenate([jnp.zeros_like(states[:1]), states[:-1]], axis=0)
    grad_log_decay = (grad_input_term * decays * prev_states).astype(jnp.bfloat16)
    return (grad_w_gate, grad_w_up, grad_w_down, grad_out_proj, grad_gate_branch, grad_log_decay, grad_input_term)
```

```python
import functools

import jax
import jax.numpy as jnp
from jax import lax
from jax.experimental import pallas as pl
from jax.experimental.pallas import tpu as pltpu
from jax.sharding import Mesh
from jax.sharding import PartitionSpec as P

BF = jnp.bfloat16
F32 = jnp.float32
I32 = jnp.int32
MESH = pl.DeviceIdType.MESH
LANES = 128
NZ = 16
CAP = 10
MSG = 24
RET = 16
ROWS = 2 * NZ * CAP
CHUNK = ROWS // 2
HALF = CHUNK // 2


def place(step):
    return max(2 * step - 1, 0) if step <= NZ // 2 else 2 * (NZ - step)


STEP_AT = [0] * NZ
for _step in range(NZ):
    STEP_AT[place(_step)] = _step


def dot(a, b):
    return jnp.dot(a, b, preferred_element_type=F32)


def dot_t(a, b):
    return lax.dot_general(a, b, (((1,), (1,)), ((), ())), preferred_element_type=F32)


def iota(shape, dim):
    return lax.broadcasted_iota(I32, shape, dim)


def landed(ref, sem):
    pltpu.make_async_copy(ref, ref, sem).wait()


class Spot:
    def __init__(self):
        self.sp = lax.axis_index("sp")
        self.tp = lax.axis_index("tp")
        self.z, self.c = self.sp // 2, self.sp % 2
        self.y, self.x = self.tp // 4, self.tp % 4

    def col(self, axis, by):
        return lax.rem(getattr(self, axis) + (by + 4), 4)

    def tpi(self, axis, by, other=0):
        a = self.col(axis, by)
        if axis == "x":
            return self.col("y", other) * 4 + a
        return a * 4 + self.col("x", other)

    def peer(self, axis, by):
        return (self.sp, self.tpi(axis, by))


def send(src, dst, ssem, rsem, dev, log):
    cp = pltpu.make_async_remote_copy(
        src_ref=src, dst_ref=dst, send_sem=ssem, recv_sem=rsem, device_id=dev, device_id_type=MESH
    )
    cp.start()
    log.append(cp)


class PlaneGather:
    def __init__(self, spot, buf, r0, n, u, ssem, rsem, log):
        self.s, self.buf, self.r0, self.n, self.u = spot, buf, r0, n, u
        self.v = "y" if u == "x" else "x"
        self.ssem, self.rsem, self.log = ssem, rsem, log
        self.sent = 0
        self.fu = (0, -1, 1, 2)

    def view(self, du, dv, half=None):
        r0, n = self.r0, self.n
        if half is not None:
            n = n // 2
            r0 = r0 + half * n
        lane = pl.multiple_of(self.s.tpi(self.u, du, dv) * LANES, LANES)
        return self.buf.at[pl.ds(r0, n), pl.ds(lane, LANES)]

    def go(self, view, axis, by, k):
        send(view, view, self.ssem.at[self.sent], self.rsem.at[k], self.s.peer(axis, by), self.log)
        self.sent += 1

    def fan(self, j):
        view = self.view(self.fu[j], 0)
        self.go(view, self.v, 1, 4 + 4 * j)
        self.go(view, self.v, -1, 5 + 4 * j)

    def stage0(self):
        view = self.view(0, 0)
        self.go(view, self.u, 1, 0)
        self.go(view, self.u, -1, 1)
        self.fan(0)

    def stage1(self):
        landed(self.view(-1, 0), self.rsem.at[0])
        self.go(self.view(-1, 0, 0), self.u, 1, 2)
        self.fan(1)
        landed(self.view(1, 0), self.rsem.at[1])
        self.go(self.view(1, 0, 1), self.u, -1, 3)
        self.fan(2)

    def relay(self, j):
        du = self.fu[j]
        landed(self.view(du, -1), self.rsem.at[4 + 4 * j])
        self.go(self.view(du, -1, 0), self.v, 1, 6 + 4 * j)
        landed(self.view(du, 1), self.rsem.at[5 + 4 * j])
        self.go(self.view(du, 1, 1), self.v, -1, 7 + 4 * j)

    def stage2(self):
        self.relay(0)

    def stage3(self):
        landed(self.view(2, 0, 0), self.rsem.at[2])
        landed(self.view(2, 0, 1), self.rsem.at[3])
        self.fan(3)

    def stage4(self):
        self.relay(1)
        self.relay(2)

    def stage5(self):
        self.relay(3)

    def stage6(self):
        for j in range(4):
            landed(self.view(self.fu[j], 2, 0), self.rsem.at[6 + 4 * j])
            landed(self.view(self.fu[j], 2, 1), self.rsem.at[7 + 4 * j])


def run_gathers(gathers):
    for k in range(7):
        for g in gathers:
            getattr(g, f"stage{k}")()


class PlaneSum:
    def __init__(self, spot, buf, r0, u, one_l, one_r, two_l, two_r, part, a_l, a_r, b_l, b_r, tmp, ssem, rsem, log):
        self.s, self.buf, self.r0, self.u = spot, buf, r0, u
        self.v = "y" if u == "x" else "x"
        self.one = (one_l, one_r)
        self.two = (two_l, two_r)
        self.part, self.a, self.b, self.tmp = part, (a_l, a_r), (b_l, b_r), tmp
        self.ssem, self.rsem, self.log = ssem, rsem, log

    def block(self, du, r0, n):
        a = self.s.col(self.u, du)
        if self.u == "x":
            return self.buf.at[:, a, pl.ds(r0, n), :]
        return self.buf.at[a, :, pl.ds(r0, n), :]

    def go(self, src, dst, axis, by, k):
        send(src, dst, self.ssem.at[k], self.rsem.at[k], self.s.peer(axis, by), self.log)

    def stage0(self):
        self.go(self.block(2, self.r0, HALF), self.one[0], self.u, 1, 0)
        self.go(self.block(2, self.r0 + HALF, HALF), self.one[1], self.u, -1, 1)

    def stage1(self):
        for side, by in ((0, 1), (1, -1)):
            landed(self.one[side], self.rsem.at[side])
            mine = self.block(by, self.r0 + side * HALF, HALF)
            mine[...] = (mine[...].astype(F32) + self.one[side][...].astype(F32)).astype(BF)
            self.go(self.block(by, self.r0, CHUNK), self.two[side], self.u, by, 2 + side)

    def stage2(self):
        landed(self.two[0], self.rsem.at[2])
        landed(self.two[1], self.rsem.at[3])
        own = self.block(0, self.r0, CHUNK)
        self.part[...] = (
            own[...].astype(F32) + self.two[0][...].astype(F32) + self.two[1][...].astype(F32)
        ).astype(BF)
        far = self.s.col(self.v, 2)
        self.go(self.part.at[far, pl.ds(0, HALF), :], self.a[0], self.v, 1, 4)
        self.go(self.part.at[far, pl.ds(HALF, HALF), :], self.a[1], self.v, -1, 5)

    def stage3(self):
        for side, by in ((0, 1), (1, -1)):
            landed(self.a[side], self.rsem.at[4 + side])
            near = self.s.col(self.v, by)
            mine = self.part.at[near, pl.ds(side * HALF, HALF), :]
            mine[...] = (mine[...].astype(F32) + self.a[side][...].astype(F32)).astype(BF)
            self.go(self.part.at[near], self.b[side], self.v, by, 6 + side)

    def stage4(self):
        landed(self.b[0], self.rsem.at[6])
        landed(self.b[1], self.rsem.at[7])
        own = self.part[self.s.col(self.v, 0)]
        total = own.astype(F32) + self.b[0][...].astype(F32) + self.b[1][...].astype(F32)
        return total.astype(BF)


def dest(spot, step, core):
    return (2 * lax.rem(spot.z + (NZ - step), NZ) + core, spot.tp)


def origin(spot, step, core):
    return (2 * lax.rem(spot.z + step, NZ) + core, spot.tp)


def group_of(expert, z):
    step = lax.rem(z - expert // 2 + NZ, NZ)
    at = jnp.where(step <= NZ // 2, jnp.maximum(2 * step - 1, 0), 2 * (NZ - step))
    return at * 2 + expert % 2


def slots_by_lane(routes_t, z):
    tok = routes_t.shape[1]
    hot = [(iota((32, tok), 0) == routes_t[k : k + 1, :]) for k in range(2)]
    both = (hot[0] | hot[1]).astype(F32).astype(BF)
    earlier = (iota((tok, tok), 0) < iota((tok, tok), 1)).astype(F32).astype(BF)
    before = dot(both, earlier)
    slot = [jnp.sum(jnp.where(h, before, 0.0), axis=0, keepdims=True).astype(I32) for h in hot]
    return [(group_of(routes_t[k : k + 1, :], z), slot[k]) for k in range(2)]


def slots_by_row(routes, z):
    tok = routes.shape[0]
    hot = [(iota((tok, 32), 1) == routes[:, k : k + 1]) for k in range(2)]
    both = (hot[0] | hot[1]).astype(F32).astype(BF)
    earlier = (iota((tok, tok), 1) < iota((tok, tok), 0)).astype(F32).astype(BF)
    before = dot(earlier, both)
    slot = [jnp.sum(jnp.where(h, before, 0.0), axis=1, keepdims=True).astype(I32) for h in hot]
    return [(group_of(routes[:, k : k + 1], z), slot[k]) for k in range(2)]


def k1_body(
    x_ref, cot_ref, routes_ref, routes_t_ref, rw_ref, wg_ref, wu_ref, wd_ref,
    rows_out, scaled_out, gp_out, hidden_out, tok_out,
    msg, arrived, xr, cr, wcat, wdv, gp, hid, terms, ret, back,
    a1l, a1r, a2l, a2r, apart, aal, aar, abl, abr,
    b1l, b1r, b2l, b2r, bpart, bal, bar, bbl, bbr,
    wsem, osem, d_s, d_r, g_s, g_r, q_s, q_r, r_s, r_r,
):
    s = Spot()
    log = []
    barrier = pltpu.get_barrier_semaphore()
    peers = 0
    for step in range(NZ):
        for core in range(2):
            if step == 0 and core == 0:
                dev = (2 * s.z + (1 - s.c), s.tp)
            elif step == 0:
                continue
            else:
                dev = dest(s, step, core)
            pl.semaphore_signal(barrier, inc=1, device_id=dev, device_id_type=MESH)
            peers += 1
    for axis in ("x", "y"):
        for by in (1, -1):
            pl.semaphore_signal(barrier, inc=1, device_id=s.peer(axis, by), device_id_type=MESH)
            peers += 1

    loads = [
        pltpu.make_async_copy(wg_ref.at[0], wcat.at[:, pl.ds(0, LANES)], wsem.at[0]),
        pltpu.make_async_copy(wu_ref.at[0], wcat.at[:, pl.ds(LANES, LANES)], wsem.at[1]),
        pltpu.make_async_copy(wd_ref.at[0], wdv, wsem.at[2]),
    ]
    for cp in loads:
        cp.start()

    by_lane = slots_by_lane(routes_t_ref[...], s.z)
    rows = [g * MSG + t for g, t in by_lane]
    at = iota((32 * MSG, LANES), 0)
    cot32 = cot_ref[...].astype(F32)
    picks = jnp.concatenate(
        [
            ((at == rows[0]) | (at == rows[1])).astype(F32).astype(BF),
            (at == rows[0] + CAP).astype(F32).astype(BF),
            (at == rows[1] + CAP).astype(F32).astype(BF),
        ],
        axis=1,
    )
    stuff = jnp.concatenate(
        [x_ref[...]] + [(rw_ref[:, k : k + 1] * cot32).astype(BF) for k in range(2)], axis=0
    )
    packed = dot(picks, stuff)
    for g in range(32):
        msg[g] = packed[g * MSG : (g + 1) * MSG, :].astype(BF)

    pl.semaphore_wait(barrier, peers)

    for chunk in range(2):
        for pos in range(chunk * 8, chunk * 8 + 8):
            step = STEP_AT[pos]
            for core in range(2):
                if step == 0:
                    if core == 1:
                        continue
                    src, dev = msg.at[1 - s.c], (2 * s.z + (1 - s.c), s.tp)
                    k = 0
                else:
                    k = 2 * pos + core
                    src, dev = msg.at[k], dest(s, step, core)
                send(src, arrived.at[2 * pos + s.c], d_s.at[k], d_r.at[chunk], dev, log)
    arrived[pl.ds(s.c, 1)] = msg[pl.ds(s.c, 1)]

    ri = iota((2 * CHUNK, 16 * MSG), 0)
    ci = iota((2 * CHUNK, 16 * MSG), 1)
    second = ri >= CHUNK
    rr = jnp.where(second, ri - CHUNK, ri)
    squeeze = (ci == (rr // CAP) * MSG + rr % CAP + jnp.where(second, CAP, 0)).astype(F32).astype(BF)

    own = pl.ds(pl.multiple_of(s.tp * LANES, LANES), LANES)
    gathers = []
    for chunk in range(2):
        waited = arrived.at[pl.ds(0, 15)] if chunk == 0 else arrived.at[pl.ds(16, 16)]
        landed(waited, d_r.at[chunk])
        block = jnp.concatenate(
            [arrived[16 * chunk + i].astype(F32) for i in range(16)], axis=0
        ).astype(BF)
        tight = dot(squeeze, block).astype(BF)
        span = pl.ds(chunk * CHUNK, CHUNK)
        xr[span, own] = tight[:CHUNK]
        cr[span, own] = tight[CHUNK:]
        pair = [
            PlaneGather(s, xr, chunk * CHUNK, CHUNK, "x", g_s.at[2 * chunk], g_r.at[2 * chunk], log),
            PlaneGather(s, cr, chunk * CHUNK, CHUNK, "y", g_s.at[2 * chunk + 1], g_r.at[2 * chunk + 1], log),
        ]
        for g in pair:
            g.stage0()
        gathers.append(pair)
    for pair in gathers:
        for k in range(1, 7):
            for g in pair:
                getattr(g, f"stage{k}")()
    for cp in loads:
        cp.wait()

    saves = [
        pltpu.make_async_copy(xr, rows_out, osem.at[0]),
        pltpu.make_async_copy(cr, scaled_out, osem.at[1]),
    ]
    for cp in saves:
        cp.start()

    sums = [
        PlaneSum(s, terms, 0, "x", a1l, a1r, a2l, a2r, apart, aal, aar, abl, abr, None, q_s.at[0], q_r.at[0], log),
        PlaneSum(s, terms, CHUNK, "y", b1l, b1r, b2l, b2r, bpart, bal, bar, bbl, bbr, None, q_s.at[1], q_r.at[1], log),
    ]
    for chunk in range(2):
        span = pl.ds(chunk * CHUNK, CHUNK)
        pre = dot(xr[span, :], wcat[...])
        gate, up = pre[:, :LANES], pre[:, LANES:]
        sig = jax.nn.sigmoid(gate)
        act = gate * sig
        slope = sig * (1.0 + gate * (1.0 - sig))
        hid[span, :] = (act * up).astype(BF)
        gh = dot_t(cr[span, :], wdv[...])
        both = jnp.concatenate([(gh * up * slope).astype(BF), (gh * act).astype(BF)], axis=1)
        gp[span, :] = both
        for far in (2, 1, 3, 0):
            for i in range(2):
                places = []
                for k in (2 * i, 2 * i + 1):
                    if chunk == 0:
                        places.append((k, s.col("x", far)))
                    else:
                        places.append((s.col("y", far), k))
                w2 = jnp.concatenate(
                    [wcat[pl.ds(pl.multiple_of((a * 4 + b) * LANES, LANES), LANES), :] for a, b in places],
                    axis=0,
                )
                t2 = dot_t(both, w2).astype(BF)
                for n, (a, b) in enumerate(places):
                    terms[a, b, span, :] = t2[:, n * LANES : (n + 1) * LANES]
            if far == 2:
                sums[chunk].stage0()
    saves += [
        pltpu.make_async_copy(gp, gp_out, osem.at[2]),
        pltpu.make_async_copy(hid, hidden_out, osem.at[3]),
    ]
    for cp in saves[2:]:
        cp.start()
    for k in range(1, 4):
        for q in sums:
            getattr(q, f"stage{k}")()

    ri = iota((16 * RET, CHUNK), 0)
    ci = iota((16 * RET, CHUNK), 1)
    spread = ((ri % RET < CAP) & (ci == (ri // RET) * CAP + ri % RET)).astype(F32).astype(BF)
    for chunk in range(2):
        total = sums[chunk].stage4()
        ret[pl.ds(16 * chunk, 16)] = dot(spread, total).astype(BF).reshape(16, RET, LANES)
        for pos in range(chunk * 8, chunk * 8 + 8):
            step = STEP_AT[pos]
            for core in range(2):
                if step == 0:
                    if core == 1:
                        continue
                    src, dev = ret.at[1 - s.c], (2 * s.z + (1 - s.c), s.tp)
                    k = 0
                else:
                    k = 2 * pos + core
                    src, dev = ret.at[k], origin(s, step, core)
                send(src, back.at[2 * pos + s.c], r_s.at[k], r_r.at[chunk], dev, log)
    back[pl.ds(s.c, 1)] = ret[pl.ds(s.c, 1)]
    by_row = slots_by_row(routes_ref[...], s.z)
    lane = iota((LANES, 32 * RET), 1)
    want = ((lane == by_row[0][0] * RET + by_row[0][1]) | (lane == by_row[1][0] * RET + by_row[1][1]))
    want = want.astype(F32).astype(BF)
    landed(back.at[pl.ds(0, 15)], r_r.at[0])
    landed(back.at[pl.ds(16, 16)], r_r.at[1])
    sums_back = dot(want, back[...].reshape(32 * RET, LANES))
    tok_out[...] = (cot32 + sums_back).astype(BF)
    for cp in log:
        cp.wait_send()
    for cp in saves:
        cp.wait()


def k1(x, cot, routes, routes_t, rw, wg, wu, wd):
    vm = pl.BlockSpec(memory_space=pltpu.VMEM)
    hb = pl.BlockSpec(memory_space=pl.ANY)
    d = 16 * LANES
    V = pltpu.VMEM
    dma = pltpu.SemaphoreType.DMA
    sums = lambda: [
        V((4, HALF, LANES), BF), V((4, HALF, LANES), BF), V((4, CHUNK, LANES), BF), V((4, CHUNK, LANES), BF),
        V((4, CHUNK, LANES), BF),
        V((HALF, LANES), BF), V((HALF, LANES), BF), V((CHUNK, LANES), BF), V((CHUNK, LANES), BF),
    ]
    return pl.pallas_call(
        k1_body,
        out_shape=[
            jax.ShapeDtypeStruct((ROWS, d), BF), jax.ShapeDtypeStruct((ROWS, d), BF),
            jax.ShapeDtypeStruct((ROWS, 2 * LANES), BF), jax.ShapeDtypeStruct((ROWS, LANES), BF),
            jax.ShapeDtypeStruct((LANES, LANES), BF),
        ],
        in_specs=[vm] * 5 + [hb] * 3,
        out_specs=[hb] * 4 + [vm],
        scratch_shapes=[
            V((32, MSG, LANES), BF), V((32, MSG, LANES), BF), V((ROWS, d), BF), V((ROWS, d), BF),
            V((d, 2 * LANES), BF), V((LANES, d), BF), V((ROWS, 2 * LANES), BF), V((ROWS, LANES), BF),
            V((4, 4, ROWS, LANES), BF), V((32, RET, LANES), BF), V((32, RET, LANES), BF),
            *sums(), *sums(),
            dma((3,)), dma((4,)), dma((32,)), dma((2,)), dma((4, 20)), dma((4, 20)),
            dma((2, 8)), dma((2, 8)), dma((32,)), dma((2,)),
        ],
        compiler_params=pltpu.CompilerParams(
            collective_id=0, has_side_effects=True, vmem_limit_bytes=56 * 1024 * 1024
        ),
        name="routed",
    )(x, cot, routes, routes_t, rw, wg, wu, wd)


SP = ("sp_0", "sp_1")


def in_one_piece(arrays, axis, split_dim, concat_dim, along):
    both = jnp.concatenate(arrays, axis=along)
    out, at, gathered = (
        lax.all_to_all(both, axis, split_axis=split_dim, concat_axis=concat_dim, tiled=True),
        0,
        [],
    )
    for a in arrays:
        gathered.append(lax.slice_in_dim(out, at, at + a.shape[along], axis=along))
        at += a.shape[along]
    return tuple(gathered)


def in_one_piece_2(arrays, axis, dim, along):
    both = jnp.concatenate(arrays, axis=along)
    out, at, gathered = (lax.all_gather(both, axis, axis=dim, tiled=True), 0, [])
    for a in arrays:
        gathered.append(lax.slice_in_dim(out, at, at + a.shape[along], axis=along))
        at += a.shape[along]
    return tuple(gathered)


def in_blocks(shard, dim, size):
    shape = shard.shape
    tiles = shard.reshape(*shape[:dim], size, shape[dim] // size, *shape[dim + 1 :])
    return jnp.moveaxis(tiles, dim, 0)


def sent_and_summed(shard, axis, dim):
    size = lax.axis_size(axis)
    tiles = lax.all_to_all(in_blocks(shard, dim, size), axis, 0, 0, tiled=True)
    return jnp.sum(tiles.astype(jnp.float32), axis=0)


def in_order(tiles, dim):
    shape = list(tiles.shape[1:])
    shape[dim] *= tiles.shape[0]
    return jnp.moveaxis(tiles, 0, dim).reshape(shape)


def copy_for_each(shard, axis):
    size = lax.axis_size(axis)
    return lax.all_to_all(
        jnp.broadcast_to(shard[None], (size, *shard.shape)), axis, 0, 0, tiled=True
    )


def gathered_copies(shard, axis, dim):
    return in_order(copy_for_each(shard, axis), dim)


def own_block(tiles, axes, order):
    inside = tiles.shape[1:]
    tiles = tiles.reshape(*(lax.axis_size(a) for a in axes), *inside)
    tiles = jnp.moveaxis(tiles, order, range(len(axes))).reshape(-1, *inside)
    for k in order:
        tiles = lax.psum_scatter(tiles, axes[k], scatter_dimension=0, tiled=True)
    return tiles[0]


def summed_rows_2(shard, axes, order, dim):
    size = lax.axis_size(axes)
    return own_block(in_blocks(shard, dim, size), axes, order)


def all_blocks(shard, axes, order):
    tiles = shard[None]
    for k in order:
        tiles = lax.all_gather(tiles, axes[k], axis=0, tiled=True)
    current = [lax.axis_size(axes[k]) for k in reversed(order)]
    tiles = tiles.reshape(*current, *shard.shape)
    turned = sorted(range(len(order)), key=lambda place: order[len(order) - 1 - place])
    return tiles.transpose(*turned, *range(len(order), tiles.ndim)).reshape(-1, *shard.shape)


def gathered_by_axis(shard, axes, order, dim):
    return in_order(all_blocks(shard, axes, order), dim)


def all_in_one(shard, axis):
    leaves = jax.tree.leaves(shard)
    order = sorted(range(len(leaves)), key=lambda k: -leaves[k].size)
    width = (1, *leaves[order[0]].shape)[-1]
    lines = [
        jnp.pad(leaves[k].reshape(-1), (0, -leaves[k].size % width)).reshape(-1, width)
        for k in order
    ]
    both, at, found = (copy_for_each(jnp.concatenate(lines), axis), 0, {})
    for k, line in zip(order, lines):
        slab = both[:, at : at + len(line)].reshape(len(both), -1)
        found[k] = slab[:, : leaves[k].size].reshape(-1, *leaves[k].shape)
        at += len(line)
    numbers = iter(range(len(leaves)))
    return jax.tree.map(lambda _: found[next(numbers)], shard)


def joined_by_halves(pieces, combine):
    while len(jax.tree.leaves(pieces)[0]) > 1:
        pieces = jax.vmap(combine)(
            *(jax.tree.map(lambda part: part[side::2], pieces) for side in (0, 1))
        )
    return jax.tree.map(lambda part: part[0], pieces)


def carried_in(shard, axis, combine, identity):
    size, mine = (lax.axis_size(axis), lax.axis_index(axis))
    passed = jnp.arange(size) > mine

    def kept(part, zero, own):
        part = jnp.where(
            passed.reshape(-1, *(1 for _ in own.shape)), part, jnp.asarray(zero, own.dtype)
        )
        return part[::-1]

    pieces = all_in_one(shard, axis)
    return joined_by_halves(jax.tree.map(kept, pieces, identity, shard), combine)


def from_behind(value, axis, steps):
    count = lax.axis_size(axis)
    leading, last = (max(0, -steps), min(count, count - steps))
    return lax.ppermute(value, axis, [(source, source + steps) for source in range(leading, last)])


def silu_parts(pre_gate):
    sigmoid_val = jax.nn.sigmoid(pre_gate)
    return (pre_gate * sigmoid_val, sigmoid_val * (1.0 + pre_gate * (1.0 - sigmoid_val)))


def combine_pair(left_pair, right_pair):
    return (left_pair[0] * right_pair[0], right_pair[0] * left_pair[1] + right_pair[1])


def compose_maps(earlier, later_map):
    return (earlier[0] * later_map[0], later_map[1] + later_map[0] * earlier[1])


def contract_rows(left_mat, right_mat):
    return lax.dot_general(
        left_mat, right_mat, (((0,), (0,)), ((), ())), preferred_element_type=jnp.float32
    )


def contract_cols(left_mat, right_mat):
    return lax.dot_general(
        left_mat, right_mat, (((1,), (1,)), ((), ())), preferred_element_type=jnp.float32
    )


def rest_shards(grad_cols, gate_branch, log_decay, states, out_proj):
    grad_tokens = gathered_copies(grad_cols, "tp", 1)
    active_gate, pullback = jax.vjp(jax.nn.gelu, gate_branch.astype(jnp.float32))
    mixed_in = (active_gate * states).astype(jnp.bfloat16)
    piece_cols = grad_tokens
    grad_out_proj = summed_rows_2(
        contract_rows(piece_cols, mixed_in).astype(jnp.bfloat16), SP, (1, 0), 0
    ).astype(jnp.float32)
    piece_cols = grad_tokens
    grad_mixed = jnp.dot(
        piece_cols, gathered_by_axis(out_proj, SP, (0, 1), 0), preferred_element_type=jnp.float32
    )
    grad_gate_branch = pullback(grad_mixed * states)[0].astype(jnp.bfloat16)
    grad_state = grad_mixed * active_gate
    decays = jnp.exp(log_decay)
    next_decay = jnp.concatenate([decays[1:], jnp.ones_like(decays[:1])], axis=0)
    span_flip, local_flip = lax.associative_scan(
        combine_pair, (jnp.flip(next_decay, 0), jnp.flip(grad_state, 0))
    )
    span_decay = jnp.flip(span_flip, 0)
    local_grad = jnp.flip(local_flip, 0)
    whole_decay = span_decay[0] * decays[0]
    entry_term = decays[0] * local_grad[0]
    carried = carried_in(
        (whole_decay, entry_term),
        SP,
        compose_maps,
        (jnp.ones_like(whole_decay), jnp.zeros_like(entry_term)),
    )
    grad_input_term = local_grad + span_decay * carried[1][None, :]
    earlier_state = from_behind(states[-1:], SP, 1)
    prev_states = jnp.concatenate([earlier_state, states[:-1]], axis=0)
    grad_log_decay = (grad_input_term * decays * prev_states).astype(jnp.bfloat16)
    return grad_out_proj, grad_gate_branch, grad_log_decay, grad_input_term


def expert_shards(moe_input, cotangent, routes, route_weights, w_gate, w_up, w_down):
    rows, scaled, gp, hidden, tok = k1(
        moe_input, cotangent, routes, routes.T, route_weights, w_gate, w_up, w_down
    )
    half = gp.shape[1] // 2
    return (
        contract_rows(rows, gp[:, :half])[None],
        contract_rows(rows, gp[:, half:])[None],
        contract_rows(hidden, scaled)[None],
        tok,
    )


def solution(mesh):
    finer = Mesh(mesh.devices.reshape(16, 2, mesh.shape["tp"]), ("sp_0", "sp_1", "tp"))
    f1 = jax.shard_map(
        expert_shards,
        mesh=mesh,
        in_specs=(
            P("sp", "tp"), P("sp", "tp"), P("sp", None), P("sp", None),
            P("sp", None, "tp"), P("sp", None, "tp"), P("sp", "tp", None),
        ),
        out_specs=(P("sp", None, "tp"), P("sp", None, "tp"), P("sp", "tp", None), P("sp", "tp")),
        check_vma=False,
    )
    f2 = jax.shard_map(
        rest_shards, mesh=finer, in_specs=(P(SP, "tp"),) * 5, out_specs=(P(SP, "tp"),) * 4, check_vma=False
    )

    def whole(
        moe_input, cotangent, routes, route_weights, gate_branch, log_decay, states, w_gate, w_up, w_down, out_proj
    ):
        gg, gu, gd, tok = f1(moe_input, cotangent, routes, route_weights, w_gate, w_up, w_down)
        return (gg, gu, gd, *f2(tok, gate_branch, log_decay, states, out_proj))

    return whole
```

```python
import functools

import jax
import jax.numpy as jnp
from jax import lax
from jax.experimental import pallas as pl
from jax.experimental.pallas import tpu as pltpu
from jax.sharding import PartitionSpec as P

BF = jnp.bfloat16
F32 = jnp.float32
I32 = jnp.int32
MESH = pl.DeviceIdType.MESH
LANES = 128
NZ = 16
CAP = 10
MSG = 24
RET = 16
ROWS = 2 * NZ * CAP
CHUNK = ROWS // 2
HALF = CHUNK // 2


def place(step):
    return max(2 * step - 1, 0) if step <= NZ // 2 else 2 * (NZ - step)


STEP_AT = [0] * NZ
for _step in range(NZ):
    STEP_AT[place(_step)] = _step


def dot(a, b):
    return jnp.dot(a, b, preferred_element_type=F32)


def dot_t(a, b):
    return lax.dot_general(a, b, (((1,), (1,)), ((), ())), preferred_element_type=F32)


def iota(shape, dim):
    return lax.broadcasted_iota(I32, shape, dim)


def landed(ref, sem):
    pltpu.make_async_copy(ref, ref, sem).wait()


class Spot:
    def __init__(self):
        self.sp = lax.axis_index("sp")
        self.tp = lax.axis_index("tp")
        self.z, self.c = self.sp // 2, self.sp % 2
        self.y, self.x = self.tp // 4, self.tp % 4

    def col(self, axis, by):
        return lax.rem(getattr(self, axis) + (by + 4), 4)

    def tpi(self, axis, by, other=0):
        a = self.col(axis, by)
        if axis == "x":
            return self.col("y", other) * 4 + a
        return a * 4 + self.col("x", other)

    def peer(self, axis, by):
        return (self.sp, self.tpi(axis, by))


def send(src, dst, ssem, rsem, dev, log):
    cp = pltpu.make_async_remote_copy(
        src_ref=src, dst_ref=dst, send_sem=ssem, recv_sem=rsem, device_id=dev, device_id_type=MESH
    )
    cp.start()
    log.append(cp)


class PlaneGather:
    def __init__(self, spot, view, u, ssem, rsem, log, total=None):
        self.s, self.block, self.u = spot, view, u
        self.v = "y" if u == "x" else "x"
        self.ssem, self.rsem, self.log, self.total = ssem, rsem, log, total
        self.sent = 0
        self.fu = (0, -1, 1, 2)

    def view(self, du, dv, half=None):
        return self.block(self.s.tpi(self.u, du, dv), half)

    def go(self, view, axis, by, k):
        ssem = self.ssem.at[self.sent] if self.total is None else self.ssem
        log = self.log if self.total is None else []
        send(view, view, ssem, self.rsem.at[k], self.s.peer(axis, by), log)
        self.sent += 1

    def fan(self, j):
        view = self.view(self.fu[j], 0)
        self.go(view, self.v, 1, 4 + 4 * j)
        self.go(view, self.v, -1, 5 + 4 * j)

    def stage0(self):
        view = self.view(0, 0)
        self.go(view, self.u, 1, 0)
        self.go(view, self.u, -1, 1)
        self.fan(0)

    def stage1(self):
        landed(self.view(-1, 0), self.rsem.at[0])
        self.go(self.view(-1, 0, 0), self.u, 1, 2)
        self.fan(1)
        landed(self.view(1, 0), self.rsem.at[1])
        self.go(self.view(1, 0, 1), self.u, -1, 3)
        self.fan(2)

    def relay(self, j):
        du = self.fu[j]
        landed(self.view(du, -1), self.rsem.at[4 + 4 * j])
        self.go(self.view(du, -1, 0), self.v, 1, 6 + 4 * j)
        landed(self.view(du, 1), self.rsem.at[5 + 4 * j])
        self.go(self.view(du, 1, 1), self.v, -1, 7 + 4 * j)

    def stage2(self):
        self.relay(0)

    def stage3(self):
        landed(self.view(2, 0, 0), self.rsem.at[2])
        landed(self.view(2, 0, 1), self.rsem.at[3])
        self.fan(3)

    def stage4(self):
        self.relay(1)
        self.relay(2)

    def stage5(self):
        self.relay(3)

    def stage6(self):
        for j in range(4):
            landed(self.view(self.fu[j], 2, 0), self.rsem.at[6 + 4 * j])
            landed(self.view(self.fu[j], 2, 1), self.rsem.at[7 + 4 * j])

    def drain(self):
        if self.total is not None:
            landed(self.total, self.ssem)


def lane_blocks(buf, r0, n):
    def view(tpi, half):
        lane = pl.ds(pl.multiple_of(tpi * LANES, LANES), LANES)
        if half is None:
            return buf.at[pl.ds(r0, n), lane]
        return buf.at[pl.ds(r0 + half * (n // 2), n // 2), lane]

    return view


def row_blocks(buf, i0, n):
    def view(tpi, half):
        if half is None:
            return buf.at[pl.ds(i0, n), tpi % 2, tpi // 2]
        return buf.at[pl.ds(i0 + half * (n // 2), n // 2), tpi % 2, tpi // 2]

    return view


class Ring:
    def __init__(self, spot, part, ssem, rsem, log):
        self.s, self.part, self.ssem, self.rsem, self.log = spot, part, ssem, rsem, log

    def at(self, by):
        return lax.rem(self.s.z + (by + NZ), NZ)

    def go(self, way, k):
        by = 1 if way == 0 else -1
        dev = (2 * self.at(by) + self.s.c, self.s.tp)
        for n, view in enumerate(self.part(self.at(-by * k))):
            send(view, view, self.ssem.at[way, n, k], self.rsem.at[way, n, k], dev, self.log)

    def start(self):
        self.go(0, 0)
        self.go(1, 0)

    def step(self, k):
        for way, by, last in ((0, 1, 8), (1, -1, 7)):
            if k < last:
                for n, view in enumerate(self.part(self.at(-by * (k + 1)))):
                    landed(view, self.rsem.at[way, n, k])
                if k + 1 < last:
                    self.go(way, k + 1)


class PlaneSum:
    def __init__(self, spot, buf, r0, u, one_l, one_r, two_l, two_r, part, a_l, a_r, b_l, b_r, tmp, ssem, rsem, log):
        self.s, self.buf, self.r0, self.u = spot, buf, r0, u
        self.v = "y" if u == "x" else "x"
        self.one = (one_l, one_r)
        self.two = (two_l, two_r)
        self.part, self.a, self.b, self.tmp = part, (a_l, a_r), (b_l, b_r), tmp
        self.ssem, self.rsem, self.log = ssem, rsem, log

    def block(self, du, r0, n):
        a = self.s.col(self.u, du)
        if self.u == "x":
            return self.buf.at[:, a, pl.ds(r0, n), :]
        return self.buf.at[a, :, pl.ds(r0, n), :]

    def go(self, src, dst, axis, by, k):
        send(src, dst, self.ssem.at[k], self.rsem.at[k], self.s.peer(axis, by), self.log)

    def stage0(self):
        self.go(self.block(2, self.r0, HALF), self.one[0], self.u, 1, 0)
        self.go(self.block(2, self.r0 + HALF, HALF), self.one[1], self.u, -1, 1)

    def stage1(self):
        for side, by in ((0, 1), (1, -1)):
            landed(self.one[side], self.rsem.at[side])
            mine = self.block(by, self.r0 + side * HALF, HALF)
            mine[...] = (mine[...].astype(F32) + self.one[side][...].astype(F32)).astype(BF)
            self.go(self.block(by, self.r0, CHUNK), self.two[side], self.u, by, 2 + side)

    def stage2(self):
        landed(self.two[0], self.rsem.at[2])
        landed(self.two[1], self.rsem.at[3])
        own = self.block(0, self.r0, CHUNK)
        self.part[...] = (
            own[...].astype(F32) + self.two[0][...].astype(F32) + self.two[1][...].astype(F32)
        ).astype(BF)
        far = self.s.col(self.v, 2)
        self.go(self.part.at[far, pl.ds(0, HALF), :], self.a[0], self.v, 1, 4)
        self.go(self.part.at[far, pl.ds(HALF, HALF), :], self.a[1], self.v, -1, 5)

    def stage3(self):
        for side, by in ((0, 1), (1, -1)):
            landed(self.a[side], self.rsem.at[4 + side])
            near = self.s.col(self.v, by)
            mine = self.part.at[near, pl.ds(side * HALF, HALF), :]
            mine[...] = (mine[...].astype(F32) + self.a[side][...].astype(F32)).astype(BF)
            self.go(self.part.at[near], self.b[side], self.v, by, 6 + side)

    def stage4(self):
        landed(self.b[0], self.rsem.at[6])
        landed(self.b[1], self.rsem.at[7])
        own = self.part[self.s.col(self.v, 0)]
        total = own.astype(F32) + self.b[0][...].astype(F32) + self.b[1][...].astype(F32)
        return total.astype(BF)


def dest(spot, step, core):
    return (2 * lax.rem(spot.z + (NZ - step), NZ) + core, spot.tp)


def origin(spot, step, core):
    return (2 * lax.rem(spot.z + step, NZ) + core, spot.tp)


def group_of(expert, z):
    step = lax.rem(z - expert // 2 + NZ, NZ)
    at = jnp.where(step <= NZ // 2, jnp.maximum(2 * step - 1, 0), 2 * (NZ - step))
    return at * 2 + expert % 2


def slots_by_lane(routes_t, z):
    tok = routes_t.shape[1]
    hot = [(iota((32, tok), 0) == routes_t[k : k + 1, :]) for k in range(2)]
    both = (hot[0] | hot[1]).astype(F32).astype(BF)
    earlier = (iota((tok, tok), 0) < iota((tok, tok), 1)).astype(F32).astype(BF)
    before = dot(both, earlier)
    slot = [jnp.sum(jnp.where(h, before, 0.0), axis=0, keepdims=True).astype(I32) for h in hot]
    return [(group_of(routes_t[k : k + 1, :], z), slot[k]) for k in range(2)]


def shifted_up(v, by, fill):
    n = v.shape[0]
    if by % 8 == 0:
        return jnp.concatenate([v[by:], jnp.full((by, v.shape[1]), fill, v.dtype)], axis=0)
    return jnp.where(iota(v.shape, 0) < n - by, pltpu.roll(v, n - by, 0), fill)


def turned(v):
    if v.shape[1] == LANES:
        low = jnp.concatenate([v[LANES:], jnp.zeros((2 * LANES - v.shape[0], LANES), F32)], axis=0)
        return jnp.concatenate([v[:LANES].T, low.T[:, : v.shape[0] - LANES]], axis=1)
    wide = jnp.concatenate([v[:, LANES:], jnp.zeros((v.shape[0], 2 * LANES - v.shape[1]), F32)], axis=1)
    return jnp.concatenate([v[:, :LANES].T, wide.T[: v.shape[1] - LANES]], axis=0)


def body(
    x_ref, cot_ref, routes_t_ref, rw_t_ref, gate_ref, ld_ref, st_ref, op_ref, wg_ref, wu_ref, wd_ref,
    rows_out, scaled_out, gp_out, hidden_out, gop_out, ggb_out, gld_out, git_out,
    msg, arrived, xr, cr, wcat, wdv, gp, hid, terms, ret, back,
    a1l, a1r, a2l, a2r, apart, aal, aar, abl, abr,
    b1l, b1r, b2l, b2r, bpart, bal, bar, bbl, bbr,
    opsib, mx, opt, spans, act_v, dact_v, dec_v, prev_v,
    toks, gt, ent, whole, lastrow, prevrow, gops, gopr,
    wsem, osem, d_s, d_r, g_s, g_r, q_s, q_r, r_s, r_r,
    o_s, o_r, ring_s, ring_r, t_s, t_r, u_s, u_r, x_s, x_r, e_s, e_r, w_s, w_r, l_s, l_r, h_s, h_r, z_s, z_r,
):
    s = Spot()
    log = []
    sibling = (2 * s.z + (1 - s.c), s.tp)
    barrier = pltpu.get_barrier_semaphore()
    peers = 1
    pl.semaphore_signal(barrier, inc=1, device_id=sibling, device_id_type=MESH)
    for step in range(1, NZ):
        for core in range(2):
            pl.semaphore_signal(barrier, inc=1, device_id=dest(s, step, core), device_id_type=MESH)
            peers += 1
    for axis in ("x", "y"):
        for by in (1, -1):
            pl.semaphore_signal(barrier, inc=1, device_id=s.peer(axis, by), device_id_type=MESH)
            peers += 1

    loads = [
        pltpu.make_async_copy(wg_ref.at[0], wcat.at[:, pl.ds(0, LANES)], wsem.at[0]),
        pltpu.make_async_copy(wu_ref.at[0], wcat.at[:, pl.ds(LANES, LANES)], wsem.at[1]),
        pltpu.make_async_copy(wd_ref.at[0], wdv, wsem.at[2]),
    ]
    for cp in loads:
        cp.start()

    def to_all(src_of, dst, ssem, rsem, chunks):
        for chunk in range(2):
            for pos in range(chunk * 8, chunk * 8 + 8):
                step = STEP_AT[pos]
                for core in range(2):
                    if step == 0 and core == 0:
                        src, dev = src_of(1 - s.c), sibling
                    elif step == 0:
                        continue
                    else:
                        src, dev = src_of(2 * pos + core), chunks(s, step, core)
                    send(src, dst(pos), ssem, rsem(chunk), dev, [])

    by_lane = slots_by_lane(routes_t_ref[...], s.z)
    rows = [g * MSG + t for g, t in by_lane]
    across = jnp.concatenate(
        [(g * RET + t).astype(F32) for g, t in by_lane] + [rw_t_ref[...], jnp.zeros((4, LANES), F32)], axis=0
    )
    down = across.T
    at = iota((32 * MSG, LANES), 0)
    cot32 = cot_ref[...].astype(F32)
    picks = jnp.concatenate(
        [
            ((at == rows[0]) | (at == rows[1])).astype(F32).astype(BF),
            (at == rows[0] + CAP).astype(F32).astype(BF),
            (at == rows[1] + CAP).astype(F32).astype(BF),
        ],
        axis=1,
    )
    stuff = jnp.concatenate(
        [x_ref[...]] + [(down[:, 2 + k : 3 + k] * cot32).astype(BF) for k in range(2)], axis=0
    )
    packed = dot(picks, stuff)
    for g in range(32):
        msg[g] = packed[g * MSG : (g + 1) * MSG, :].astype(BF)

    pl.semaphore_wait(barrier, peers)

    to_all(lambda k: msg.at[k], lambda pos: arrived.at[2 * pos + s.c], d_s, lambda c: d_r.at[c], dest)
    send(op_ref, opsib, o_s, o_r, sibling, log)
    arrived[pl.ds(s.c, 1)] = msg[pl.ds(s.c, 1)]

    gate = gate_ref[...].astype(F32)
    states = st_ref[...]
    root = 0.7978845608028654
    th = jnp.tanh(root * (gate + 0.044715 * (gate * gate * gate)))
    act_g = 0.5 * gate * (1.0 + th)
    act_v[...] = act_g
    dact_v[...] = 0.5 * (1.0 + th) + 0.5 * gate * (1.0 - th * th) * (root * (1.0 + 3 * 0.044715 * (gate * gate)))
    lanes_z = pl.ds(pl.multiple_of(s.z * LANES, LANES), LANES)
    mx[:, lanes_z] = turned((act_g * states).astype(BF).astype(F32)).astype(BF)
    landed(opsib, o_r)
    mine, other = op_ref[...].astype(F32), opsib[...].astype(F32)
    first = s.c == 0
    both = jnp.concatenate([jnp.where(first, mine, other), jnp.where(first, other, mine)], axis=0)
    both = turned(both)
    halfw = both.shape[0] // 2
    oprows = pl.ds(pl.multiple_of(s.c * halfw, 16), halfw)
    opt[oprows, lanes_z] = jnp.where(first, both[:halfw], both[halfw:]).astype(BF)

    def ring_part(z):
        lane = pl.ds(pl.multiple_of(z * LANES, LANES), LANES)
        return (opt.at[oprows, lane], mx.at[:, lane])

    ring = Ring(s, ring_part, ring_s, ring_r, log)
    ring.start()

    decays = jnp.exp(ld_ref[...])
    dec_v[...] = decays
    span = shifted_up(decays, 1, 1.0)
    for k in range(7):
        spans[k] = span
        span = span * shifted_up(span, 2**k, 1.0)
    spans[7] = span
    whole[s.sp] = span[0:1] * decays[0:1]
    lastrow[0] = states[127:128]
    to_all(lambda k: whole.at[s.sp], lambda pos: whole.at[s.sp], w_s, lambda c: w_r, dest)
    send(lastrow, prevrow, l_s, l_r, (lax.rem(s.sp + 1, 32), s.tp), log)

    ri = iota((2 * CHUNK, 16 * MSG), 0)
    ci = iota((2 * CHUNK, 16 * MSG), 1)
    second = ri >= CHUNK
    rr = jnp.where(second, ri - CHUNK, ri)
    squeeze = (ci == (rr // CAP) * MSG + rr % CAP + jnp.where(second, CAP, 0)).astype(F32).astype(BF)

    own = pl.ds(pl.multiple_of(s.tp * LANES, LANES), LANES)
    gathers = []
    for chunk in range(2):
        waited = arrived.at[pl.ds(0, 15)] if chunk == 0 else arrived.at[pl.ds(16, 16)]
        landed(waited, d_r.at[chunk])
        block = jnp.concatenate(
            [arrived[16 * chunk + i].astype(F32) for i in range(16)], axis=0
        ).astype(BF)
        tight = dot(squeeze, block).astype(BF)
        part = pl.ds(chunk * CHUNK, CHUNK)
        xr[part, own] = tight[:CHUNK]
        cr[part, own] = tight[CHUNK:]
        pair = []
        for n, (buf, u) in enumerate(((xr, "x"), (cr, "y"))):
            total = buf.at[part, pl.ds(0, 15 * LANES)]
            view = lane_blocks(buf, chunk * CHUNK, CHUNK)
            pair.append(PlaneGather(s, view, u, g_s.at[2 * chunk + n], g_r.at[2 * chunk + n], log, total))
        for g in pair:
            g.stage0()
        gathers.append(pair)
    for n, pair in enumerate(gathers):
        for k in range(1, 7):
            for g in pair:
                getattr(g, f"stage{k}")()
            if k % 2 == 0:
                ring.step(3 * n + k // 2 - 1)
    for cp in loads:
        cp.wait()

    saves = [
        pltpu.make_async_copy(xr, rows_out, osem.at[0]),
        pltpu.make_async_copy(cr, scaled_out, osem.at[1]),
    ]
    for cp in saves:
        cp.start()

    sums = [
        PlaneSum(s, terms, 0, "x", a1l, a1r, a2l, a2r, apart, aal, aar, abl, abr, None, q_s.at[0], q_r.at[0], log),
        PlaneSum(s, terms, CHUNK, "y", b1l, b1r, b2l, b2r, bpart, bal, bar, bbl, bbr, None, q_s.at[1], q_r.at[1], log),
    ]
    for chunk in range(2):
        part = pl.ds(chunk * CHUNK, CHUNK)
        pre = dot(xr[part, :], wcat[...])
        pgate, up = pre[:, :LANES], pre[:, LANES:]
        sig = jax.nn.sigmoid(pgate)
        act = pgate * sig
        slope = sig * (1.0 + pgate * (1.0 - sig))
        hid[part, :] = (act * up).astype(BF)
        gh = dot_t(cr[part, :], wdv[...])
        grads = jnp.concatenate([(gh * up * slope).astype(BF), (gh * act).astype(BF)], axis=1)
        gp[part, :] = grads
        for far in (2, 1, 3, 0):
            for i in range(2):
                places = []
                for k in (2 * i, 2 * i + 1):
                    if chunk == 0:
                        places.append((k, s.col("x", far)))
                    else:
                        places.append((s.col("y", far), k))
                w2 = jnp.concatenate(
                    [wcat[pl.ds(pl.multiple_of((a * 4 + b) * LANES, LANES), LANES), :] for a, b in places],
                    axis=0,
                )
                t2 = dot_t(grads, w2).astype(BF)
                for n, (a, b) in enumerate(places):
                    terms[a, b, part, :] = t2[:, n * LANES : (n + 1) * LANES]
            if far == 2:
                sums[chunk].stage0()
    saves += [
        pltpu.make_async_copy(gp, gp_out, osem.at[2]),
        pltpu.make_async_copy(hid, hidden_out, osem.at[3]),
    ]
    for cp in saves[2:]:
        cp.start()
    for k in range(1, 4):
        for q in sums:
            getattr(q, f"stage{k}")()
        if k < 3:
            ring.step(5 + k)
    send(opt.at[oprows, :], opt.at[oprows, :], h_s, h_r, sibling, log)

    ri = iota((16 * RET, CHUNK), 0)
    ci = iota((16 * RET, CHUNK), 1)
    spread = ((ri % RET < CAP) & (ci == (ri // RET) * CAP + ri % RET)).astype(F32).astype(BF)
    for chunk in range(2):
        total = sums[chunk].stage4()
        ret[pl.ds(16 * chunk, 16)] = dot(spread, total).astype(BF).reshape(16, RET, LANES)
    to_all(lambda k: ret.at[k], lambda pos: back.at[2 * pos + s.c], r_s, lambda c: r_r.at[c], origin)
    back[pl.ds(s.c, 1)] = ret[pl.ds(s.c, 1)]
    lane = iota((LANES, 32 * RET), 1)
    spots = down[:, 0:2].astype(I32)
    want = ((lane == spots[:, 0:1]) | (lane == spots[:, 1:2])).astype(F32).astype(BF)
    landed(back.at[pl.ds(0, 15)], r_r.at[0])
    landed(back.at[pl.ds(16, 16)], r_r.at[1])
    grown = dot(want, back[...].reshape(32 * RET, LANES))
    tok = (cot32 + grown).astype(BF)
    toks[:, own] = tok

    rows_of = toks.shape[0]
    fans = []
    for n, u in enumerate(("x", "y")):
        r0, cnt = n * (rows_of // 2), rows_of // 2
        total = toks.at[pl.ds(r0, cnt), pl.ds(0, 15 * LANES)]
        fans.append(PlaneGather(s, lane_blocks(toks, r0, cnt), u, t_s.at[n], t_r.at[n], log, total))
    for f in fans:
        f.stage0()
    inplace = s.z == s.tp
    odd = s.z % 2
    for q in range(8):
        col = 2 * q + odd
        src = toks.at[pl.ds(16 * q, 16), own]
        keep = jnp.logical_and(inplace, col == s.tp)

        @pl.when(jnp.logical_not(keep))
        def _():
            send(src, gt.at[s.z // 2, odd, q], x_s.at[q], x_r.at[s.z // 2], (2 * s.tp + s.c, col), [])

        @pl.when(keep)
        def _():
            gt[s.z // 2, odd, q] = src[...]

    turns = [
        PlaneGather(s, row_blocks(gt, 4 * n, 4), u, u_s.at[n], u_r.at[n], log)
        for n, u in enumerate(("x", "y"))
    ]
    for k in range(1, 4):
        for f in fans:
            getattr(f, f"stage{k}")()
    for i in range(8):
        keep = jnp.logical_and(inplace, s.z // 2 == i)

        @pl.when(jnp.logical_not(keep))
        def _():
            landed(gt.at[i, s.tp % 2, s.tp // 2], x_r.at[i])

    for f in turns:
        f.stage0()
    for k in range(4, 7):
        for f in fans:
            getattr(f, f"stage{k}")()
    landed(opt.at[pl.ds(pl.multiple_of((1 - s.c) * halfw, 16), halfw), :], h_r)
    gm = dot_t(toks[...], opt[...])
    act_g, decays, states = act_v[...], dec_v[...], st_ref[...]
    local = gm * act_g
    for k in range(7):
        local = local + spans[k] * shifted_up(local, 2**k, 0.0)
    ent[s.sp] = decays[0:1] * local[0:1]
    to_all(lambda k: ent.at[s.sp], lambda pos: ent.at[s.sp], e_s, lambda c: e_r, dest)
    ggb_out[...] = (gm * states * dact_v[...]).astype(BF)
    for k in range(1, 7):
        for f in turns:
            getattr(f, f"stage{k}")()
    gops[...] = dot(mx[...], gt[...].reshape(16 * LANES, LANES))
    send(gops, gopr, z_s, z_r, sibling, log)

    landed(whole.at[pl.ds(0, 31)], w_r)
    landed(prevrow, l_r)
    prev = jnp.where(s.sp == 0, 0.0, prevrow[0])
    prev = jnp.where(iota(states.shape, 0) == 0, prev, pltpu.roll(states, 1, 0)) * decays
    landed(ent.at[pl.ds(0, 31)], e_r)
    carry = jnp.zeros_like(decays[0:1])
    for k in range(31, 0, -1):
        carry = jnp.where(s.sp < k, ent[k] + whole[k] * carry, carry)
    full = local + spans[7] * carry
    git_out[...] = full
    gld_out[...] = (full * prev).astype(BF)
    landed(gopr, z_r)
    gop = turned(gops[...] + gopr[...])
    gop_out[...] = jnp.where(first, gop[:64], gop[64:])

    for cp in log:
        cp.wait_send()
    for q in range(8):
        keep = jnp.logical_and(inplace, 2 * q + odd == s.tp)

        @pl.when(jnp.logical_not(keep))
        def _():
            landed(toks.at[pl.ds(16 * q, 16), own], x_s.at[q])

    for g in gathers[0] + gathers[1] + fans + turns:
        g.drain()
    landed(msg.at[pl.ds(0, 31)], d_s)
    landed(ret.at[pl.ds(0, 31)], r_s)
    landed(ent.at[pl.ds(0, 31)], e_s)
    landed(whole.at[pl.ds(0, 31)], w_s)
    for cp in saves:
        cp.wait()


def step(x, cot, routes, rw, gate, ld, st, wg, wu, wd, op):
    vm = pl.BlockSpec(memory_space=pltpu.VMEM)
    hb = pl.BlockSpec(memory_space=pl.ANY)
    d = 16 * LANES
    w = gate.shape[1]
    V = pltpu.VMEM
    dma = pltpu.SemaphoreType.DMA
    S = jax.ShapeDtypeStruct
    sums = lambda: [
        V((4, HALF, LANES), BF), V((4, HALF, LANES), BF), V((4, CHUNK, LANES), BF), V((4, CHUNK, LANES), BF),
        V((4, CHUNK, LANES), BF),
        V((HALF, LANES), BF), V((HALF, LANES), BF), V((CHUNK, LANES), BF), V((CHUNK, LANES), BF),
    ]
    rows, scaled, gp, hidden, gop, ggb, gld, git = pl.pallas_call(
        body,
        out_shape=[
            S((ROWS, d), BF), S((ROWS, d), BF), S((ROWS, 2 * LANES), BF), S((ROWS, LANES), BF),
            S(op.shape, F32), S(gate.shape, BF), S(gate.shape, BF), S(gate.shape, F32),
        ],
        in_specs=[vm] * 8 + [hb] * 3,
        out_specs=[hb] * 4 + [vm] * 4,
        scratch_shapes=[
            V((32, MSG, LANES), BF), V((32, MSG, LANES), BF), V((ROWS, d), BF), V((ROWS, d), BF),
            V((d, 2 * LANES), BF), V((LANES, d), BF), V((ROWS, 2 * LANES), BF), V((ROWS, LANES), BF),
            V((4, 4, ROWS, LANES), BF), V((32, RET, LANES), BF), V((32, RET, LANES), BF),
            *sums(), *sums(),
            V(op.shape, BF), V((w, d), BF), V((w, d), BF), V((8, LANES, w), F32),
            V((LANES, w), F32), V((LANES, w), F32), V((LANES, w), F32), V((LANES, w), F32),
            V((LANES, d), BF), V((8, 2, 8, 16, LANES), BF), V((32, 1, w), F32), V((32, 1, w), F32),
            V((1, 1, w), F32), V((1, 1, w), F32), V((w, LANES), F32), V((w, LANES), F32),
            dma((3,)), dma((4,)), dma, dma((2,)), dma((4,)), dma((4, 20)),
            dma((2, 8)), dma((2, 8)), dma, dma((2,)),
            dma, dma, dma((2, 2, 8)), dma((2, 2, 8)), dma((2,)), dma((2, 20)), dma((2, 20)), dma((2, 20)),
            dma((8,)), dma((8,)), dma, dma, dma, dma, dma, dma, dma, dma, dma, dma,
        ],
        compiler_params=pltpu.CompilerParams(
            collective_id=0, has_side_effects=True, vmem_limit_bytes=56 * 1024 * 1024
        ),
        name="whole_step",
    )(x, cot, routes.T, rw.T, gate, ld, st, op, wg, wu, wd)

    def rows_by(a, b):
        return lax.dot_general(a, b, (((0,), (0,)), ((), ())), preferred_element_type=F32)

    return (
        rows_by(rows, gp[:, :LANES])[None], rows_by(rows, gp[:, LANES:])[None], rows_by(hidden, scaled)[None],
        gop, ggb, gld, git,
    )


def solution(mesh):
    both, rows = P("sp", "tp"), P("sp", None)
    last, middle = P("sp", None, "tp"), P("sp", "tp", None)
    return jax.shard_map(
        step,
        mesh=mesh,
        in_specs=(both, both, rows, rows, both, both, both, last, last, middle, both),
        out_specs=(last, last, middle, both, both, both, both),
        check_vma=False,
    )
```

```python
import functools

import jax
import jax.numpy as jnp
from jax import lax
from jax.experimental import pallas as pl
from jax.experimental.pallas import tpu as pltpu
from jax.sharding import PartitionSpec as P

BF = jnp.bfloat16
F32 = jnp.float32
I32 = jnp.int32
MESH = pl.DeviceIdType.MESH
LANES = 128
NZ = 16
CAP = 10
MSG = 24
RET = 16
ROWS = 2 * NZ * CAP
CHUNK = ROWS // 2
HALF = CHUNK // 2
VMEM_MIB = 30


def place(step):
    return max(2 * step - 1, 0) if step <= NZ // 2 else 2 * (NZ - step)


STEP_AT = [0] * NZ
for _step in range(NZ):
    STEP_AT[place(_step)] = _step


def dot(a, b):
    return jnp.dot(a, b, preferred_element_type=F32)


def dot_t(a, b):
    return lax.dot_general(a, b, (((1,), (1,)), ((), ())), preferred_element_type=F32)


def iota(shape, dim):
    return lax.broadcasted_iota(I32, shape, dim)


def landed(ref, sem):
    pltpu.make_async_copy(ref, ref, sem).wait()


class Spot:
    def __init__(self):
        self.sp = lax.axis_index("sp")
        self.tp = lax.axis_index("tp")
        self.z, self.c = self.sp // 2, self.sp % 2
        self.y, self.x = self.tp // 4, self.tp % 4

    def col(self, axis, by):
        return lax.rem(getattr(self, axis) + (by + 4), 4)

    def tpi(self, axis, by, other=0):
        a = self.col(axis, by)
        if axis == "x":
            return self.col("y", other) * 4 + a
        return a * 4 + self.col("x", other)

    def peer(self, axis, by):
        return (self.sp, self.tpi(axis, by))


def send(src, dst, ssem, rsem, dev, log):
    cp = pltpu.make_async_remote_copy(
        src_ref=src, dst_ref=dst, send_sem=ssem, recv_sem=rsem, device_id=dev, device_id_type=MESH
    )
    cp.start()
    log.append(cp)


class PlaneGather:
    def __init__(self, spot, view, u, ssem, rsem, log, total=None):
        self.s, self.block, self.u = spot, view, u
        self.v = "y" if u == "x" else "x"
        self.ssem, self.rsem, self.log, self.total = ssem, rsem, log, total
        self.sent = 0
        self.fu = (0, -1, 1, 2)

    def view(self, du, dv, half=None):
        return self.block(self.s.tpi(self.u, du, dv), half)

    def go(self, view, axis, by, k):
        ssem = self.ssem.at[self.sent] if self.total is None else self.ssem
        log = self.log if self.total is None else []
        send(view, view, ssem, self.rsem.at[k], self.s.peer(axis, by), log)
        self.sent += 1

    def fan(self, j):
        view = self.view(self.fu[j], 0)
        self.go(view, self.v, 1, 4 + 4 * j)
        self.go(view, self.v, -1, 5 + 4 * j)

    def stage0(self):
        view = self.view(0, 0)
        self.go(view, self.u, 1, 0)
        self.go(view, self.u, -1, 1)

    def stage1(self):
        landed(self.view(-1, 0), self.rsem.at[0])
        self.go(self.view(-1, 0, 0), self.u, 1, 2)
        self.fan(1)
        landed(self.view(1, 0), self.rsem.at[1])
        self.go(self.view(1, 0, 1), self.u, -1, 3)
        self.fan(2)

    def relay(self, j):
        du = self.fu[j]
        landed(self.view(du, -1), self.rsem.at[4 + 4 * j])
        self.go(self.view(du, -1, 0), self.v, 1, 6 + 4 * j)
        landed(self.view(du, 1), self.rsem.at[5 + 4 * j])
        self.go(self.view(du, 1, 1), self.v, -1, 7 + 4 * j)

    def stage2(self):
        self.relay(0)

    def stage3(self):
        landed(self.view(2, 0, 0), self.rsem.at[2])
        landed(self.view(2, 0, 1), self.rsem.at[3])
        self.fan(3)

    def stage4(self):
        self.relay(1)
        self.relay(2)

    def stage5(self):
        self.relay(3)

    def stage6(self):
        for j in range(4):
            landed(self.view(self.fu[j], 2, 0), self.rsem.at[6 + 4 * j])
            landed(self.view(self.fu[j], 2, 1), self.rsem.at[7 + 4 * j])

    def drain(self):
        if self.total is not None:
            landed(self.total, self.ssem)


class PlaneCast:
    def __init__(self, spot, view, ssem, rsem):
        self.s, self.view, self.ssem, self.rsem = spot, view, ssem, rsem
        self.log = []
        self.moves = [(dy, dx) for dy in (2, 1, 3, 0) for dx in (2, 1, 3, 0) if dy or dx]

    def start(self):
        block = self.view(self.s.tp, None)
        for k, (dy, dx) in enumerate(self.moves):
            dev = (self.s.sp, self.s.tpi("y", dy, dx))
            send(block, block, self.ssem.at[k], self.rsem.at[k], dev, self.log)

    def finish(self):
        for k, (dy, dx) in enumerate(self.moves):
            landed(self.view(self.s.tpi("y", -dy, -dx), None), self.rsem.at[k])

    def drain(self):
        for cp in self.log:
            cp.wait_send()


def lane_blocks(buf, r0, n):
    def view(tpi, half):
        lane = pl.ds(pl.multiple_of(tpi * LANES, LANES), LANES)
        if half is None:
            return buf.at[pl.ds(r0, n), lane]
        return buf.at[pl.ds(r0 + half * (n // 2), n // 2), lane]

    return view


def row_blocks(buf, i0, n):
    def view(tpi, half):
        if half is None:
            return buf.at[pl.ds(i0, n), tpi % 2, tpi // 2]
        return buf.at[pl.ds(i0 + half * (n // 2), n // 2), tpi % 2, tpi // 2]

    return view


class Ring:
    def __init__(self, spot, part, ssem, rsem, log):
        self.s, self.part, self.ssem, self.rsem, self.log = spot, part, ssem, rsem, log

    def at(self, by):
        return lax.rem(self.s.z + (by + NZ), NZ)

    def go(self, way, k):
        by = 1 if way == 0 else -1
        dev = (2 * self.at(by) + self.s.c, self.s.tp)
        for n, view in enumerate(self.part(self.at(-by * k))):
            send(view, view, self.ssem.at[way, n, k], self.rsem.at[way, n, k], dev, self.log)

    def start(self):
        self.go(0, 0)
        self.go(1, 0)

    def step(self, k):
        for way, by, last in ((0, 1, 8), (1, -1, 7)):
            if k < last:
                for n, view in enumerate(self.part(self.at(-by * (k + 1)))):
                    landed(view, self.rsem.at[way, n, k])
                if k + 1 < last:
                    self.go(way, k + 1)


class PlaneSum:
    def __init__(self, spot, buf, r0, u, one_l, one_r, two_l, two_r, part, a_l, a_r, b_l, b_r, tmp, ssem, rsem, log):
        self.s, self.buf, self.r0, self.u = spot, buf, r0, u
        self.v = "y" if u == "x" else "x"
        self.one = (one_l, one_r)
        self.two = (two_l, two_r)
        self.part, self.a, self.b, self.tmp = part, (a_l, a_r), (b_l, b_r), tmp
        self.ssem, self.rsem, self.log = ssem, rsem, log

    def block(self, du, r0, n):
        a = self.s.col(self.u, du)
        if self.u == "x":
            return self.buf.at[:, a, pl.ds(r0, n), :]
        return self.buf.at[a, :, pl.ds(r0, n), :]

    def go(self, src, dst, axis, by, k):
        send(src, dst, self.ssem.at[k], self.rsem.at[k], self.s.peer(axis, by), self.log)

    def stage0(self):
        self.go(self.block(2, self.r0, HALF), self.one[0], self.u, 1, 0)
        self.go(self.block(2, self.r0 + HALF, HALF), self.one[1], self.u, -1, 1)

    def stage1(self):
        for side, by in ((0, 1), (1, -1)):
            landed(self.one[side], self.rsem.at[side])
            mine = self.block(by, self.r0 + side * HALF, HALF)
            mine[...] = (mine[...].astype(F32) + self.one[side][...].astype(F32)).astype(BF)
            self.go(self.block(by, self.r0, CHUNK), self.two[side], self.u, by, 2 + side)

    def stage2(self):
        landed(self.two[0], self.rsem.at[2])
        landed(self.two[1], self.rsem.at[3])
        own = self.block(0, self.r0, CHUNK)
        self.part[...] = (
            own[...].astype(F32) + self.two[0][...].astype(F32) + self.two[1][...].astype(F32)
        ).astype(BF)
        far = self.s.col(self.v, 2)
        self.go(self.part.at[far, pl.ds(0, HALF), :], self.a[0], self.v, 1, 4)
        self.go(self.part.at[far, pl.ds(HALF, HALF), :], self.a[1], self.v, -1, 5)

    def stage3(self):
        for side, by in ((0, 1), (1, -1)):
            landed(self.a[side], self.rsem.at[4 + side])
            near = self.s.col(self.v, by)
            mine = self.part.at[near, pl.ds(side * HALF, HALF), :]
            mine[...] = (mine[...].astype(F32) + self.a[side][...].astype(F32)).astype(BF)
            self.go(self.part.at[near], self.b[side], self.v, by, 6 + side)

    def stage4(self):
        landed(self.b[0], self.rsem.at[6])
        landed(self.b[1], self.rsem.at[7])
        own = self.part[self.s.col(self.v, 0)]
        total = own.astype(F32) + self.b[0][...].astype(F32) + self.b[1][...].astype(F32)
        return total.astype(BF)


def dest(spot, step, core):
    return (2 * lax.rem(spot.z + (NZ - step), NZ) + core, spot.tp)


def origin(spot, step, core):
    return (2 * lax.rem(spot.z + step, NZ) + core, spot.tp)


def group_of(expert, z):
    step = lax.rem(z - expert // 2 + NZ, NZ)
    at = jnp.where(step <= NZ // 2, jnp.maximum(2 * step - 1, 0), 2 * (NZ - step))
    return at * 2 + expert % 2


def slots_by_lane(routes_t, z):
    tok = routes_t.shape[1]
    hot = [(iota((32, tok), 0) == routes_t[k : k + 1, :]) for k in range(2)]
    both = (hot[0] | hot[1]).astype(F32).astype(BF)
    earlier = (iota((tok, tok), 0) < iota((tok, tok), 1)).astype(F32).astype(BF)
    before = dot(both, earlier)
    slot = [jnp.sum(jnp.where(h, before, 0.0), axis=0, keepdims=True).astype(I32) for h in hot]
    return [(group_of(routes_t[k : k + 1, :], z), slot[k]) for k in range(2)]


def dot_0(a, b):
    return lax.dot_general(a, b, (((0,), (0,)), ((), ())), preferred_element_type=F32)


def shifted_up(v, by, fill):
    n = v.shape[1]
    return jnp.where(iota(v.shape, 1) < n - by, pltpu.roll(v, n - by, 1), fill)


def turned(v):
    if v.shape[1] == LANES:
        low = jnp.concatenate([v[LANES:], jnp.zeros((2 * LANES - v.shape[0], LANES), F32)], axis=0)
        return jnp.concatenate([v[:LANES].T, low.T[:, : v.shape[0] - LANES]], axis=1)
    wide = jnp.concatenate([v[:, LANES:], jnp.zeros((v.shape[0], 2 * LANES - v.shape[1]), F32)], axis=1)
    return jnp.concatenate([v[:, :LANES].T, wide.T[: v.shape[1] - LANES]], axis=0)


def body(
    x_in, cot_in, routes_in, rw_in, gate_in, ld_in, st_in, op_in, wg_ref, wu_ref, wd_ref,
    gg_out, gu_out, gd_out, gop_out, ggb_out, gld_out, git_out,
    x_ref, cot_ref, routes_t_ref, rw_t_ref, gate_ref, ld_ref, st_ref, op_ref,
    msg, arrived, xr, cr, wcat, wdv, gp, hid, terms, ret, back,
    a1l, a1r, a2l, a2r, apart, aal, aar, abl, abr,
    b1l, b1r, b2l, b2r, bpart, bal, bar, bbl, bbr,
    opsib, mx, opt, spans, act_v, dact_v, dec_v,
    toks, gt, ent, whole, lastrow, prevrow, gops, gopr,
    isem, wsem, d_s, d_r, g_s, g_r, q_s, q_r, r_s, r_r,
    o_s, o_r, ring_s, ring_r, t_s, t_r, u_s, u_r, x_s, x_r, e_s, e_r, w_s, w_r, l_s, l_r, h_s, h_r, z_s, z_r,
):
    inputs = [
        pltpu.make_async_copy(src, dst, isem.at[k])
        for k, (src, dst) in enumerate(
            (
                (routes_in, routes_t_ref), (rw_in, rw_t_ref), (x_in, x_ref), (cot_in, cot_ref),
                (op_in, op_ref), (gate_in, gate_ref), (st_in, st_ref), (ld_in, ld_ref),
            )
        )
    ]
    for cp in inputs:
        cp.start()
    s = Spot()
    log = []
    sibling = (2 * s.z + (1 - s.c), s.tp)
    barrier = pltpu.get_barrier_semaphore()
    peers = 1
    pl.semaphore_signal(barrier, inc=1, device_id=sibling, device_id_type=MESH)
    for step in range(1, NZ):
        for core in range(2):
            pl.semaphore_signal(barrier, inc=1, device_id=dest(s, step, core), device_id_type=MESH)
            peers += 1
    for axis in ("x", "y"):
        for by in (1, -1):
            pl.semaphore_signal(barrier, inc=1, device_id=s.peer(axis, by), device_id_type=MESH)
            peers += 1

    loads = [
        pltpu.make_async_copy(wg_ref.at[0], wcat.at[:, pl.ds(0, LANES)], wsem.at[0]),
        pltpu.make_async_copy(wu_ref.at[0], wcat.at[:, pl.ds(LANES, LANES)], wsem.at[1]),
        pltpu.make_async_copy(wd_ref.at[0], wdv, wsem.at[2]),
    ]
    for cp in loads:
        cp.start()

    def to_all(src_of, dst, ssem, rsem, target, chunk):
        for pos in range(chunk * 8, chunk * 8 + 8):
            step = STEP_AT[pos]
            for turn in range(2):
                core = (s.c, 1 - s.c)[turn]
                if step == 0:
                    if turn == 0:
                        continue
                    dev = sibling
                else:
                    dev = target(s, step, core)
                send(src_of(2 * pos + core), dst(pos), ssem, rsem, dev, [])

    for cp in inputs[:2]:
        cp.wait()
    by_lane = slots_by_lane(routes_t_ref[...], s.z)
    rows = [g * MSG + t for g, t in by_lane]
    across = jnp.concatenate(
        [(g * RET + t).astype(F32) for g, t in by_lane] + [rw_t_ref[...], jnp.zeros((4, LANES), F32)], axis=0
    )
    down = across.T
    at = iota((32 * MSG, LANES), 0)
    for cp in inputs[2:4]:
        cp.wait()
    cot32 = cot_ref[...].astype(F32)
    picks = jnp.concatenate(
        [
            ((at == rows[0]) | (at == rows[1])).astype(F32).astype(BF),
            (at == rows[0] + CAP).astype(F32).astype(BF),
            (at == rows[1] + CAP).astype(F32).astype(BF),
        ],
        axis=1,
    )
    stuff = jnp.concatenate(
        [x_ref[...]] + [(down[:, 2 + k : 3 + k] * cot32).astype(BF) for k in range(2)], axis=0
    )
    packed = dot(picks, stuff)
    for g in range(32):
        msg[g] = packed[g * MSG : (g + 1) * MSG, :].astype(BF)

    pl.semaphore_wait(barrier, peers)

    for chunk in range(2):
        to_all(lambda k: msg.at[k], lambda pos: arrived.at[2 * pos + s.c], d_s, d_r.at[chunk], dest, chunk)
    for cp in inputs[4:]:
        cp.wait()
    send(op_ref, opsib, o_s, o_r, sibling, log)
    arrived[pl.ds(s.c, 1)] = msg[pl.ds(s.c, 1)]

    gate = gate_ref[...].astype(F32)
    states = st_ref[...]
    root = 0.7978845608028654
    th = jnp.tanh(root * (gate + 0.044715 * (gate * gate * gate)))
    act_g = 0.5 * gate * (1.0 + th)
    act_v[...] = act_g
    dact_v[...] = 0.5 * (1.0 + th) + 0.5 * gate * (1.0 - th * th) * (root * (1.0 + 3 * 0.044715 * (gate * gate)))
    lanes_z = pl.ds(pl.multiple_of(s.z * LANES, LANES), LANES)
    mx[:, lanes_z] = (act_g * states).astype(BF)
    landed(opsib, o_r)
    mine, other = op_ref[...].astype(F32), opsib[...].astype(F32)
    first = s.c == 0
    both = jnp.concatenate([jnp.where(first, mine, other), jnp.where(first, other, mine)], axis=0)
    both = turned(both)
    halfw = both.shape[0] // 2
    oprows = pl.ds(pl.multiple_of(s.c * halfw, 16), halfw)
    opt[oprows, lanes_z] = jnp.where(first, both[:halfw], both[halfw:]).astype(BF)

    def ring_part(z):
        lane = pl.ds(pl.multiple_of(z * LANES, LANES), LANES)
        return (opt.at[oprows, lane], mx.at[:, lane])

    ring = Ring(s, ring_part, ring_s, ring_r, log)
    ring.start()

    decays = jnp.exp(ld_ref[...])
    dec_v[...] = decays
    span = shifted_up(decays, 1, 1.0)
    for k in range(7):
        spans[k] = span
        span = span * shifted_up(span, 2**k, 1.0)
    spans[7] = span
    whole[s.sp] = turned(span * decays)[0:1]
    lastrow[0] = turned(states)[LANES - 1 :]
    for chunk in range(2):
        to_all(lambda k: whole.at[s.sp], lambda pos: whole.at[s.sp], w_s, w_r, dest, chunk)
    send(lastrow, prevrow, l_s, l_r, (lax.rem(s.sp + 1, 32), s.tp), log)

    ri = iota((2 * CHUNK, 16 * MSG), 0)
    ci = iota((2 * CHUNK, 16 * MSG), 1)
    second = ri >= CHUNK
    rr = jnp.where(second, ri - CHUNK, ri)
    squeeze = (ci == (rr // CAP) * MSG + rr % CAP + jnp.where(second, CAP, 0)).astype(F32).astype(BF)

    own = pl.ds(pl.multiple_of(s.tp * LANES, LANES), LANES)
    gathers = []
    sums = [
        PlaneSum(s, terms, 0, "x", a1l, a1r, a2l, a2r, apart, aal, aar, abl, abr, None, q_s.at[0], q_r.at[0], log),
        PlaneSum(s, terms, CHUNK, "y", b1l, b1r, b2l, b2r, bpart, bal, bar, bbl, bbr, None, q_s.at[1], q_r.at[1], log),
    ]
    ri = iota((16 * RET, CHUNK), 0)
    ci = iota((16 * RET, CHUNK), 1)
    spread = ((ri % RET < CAP) & (ci == (ri // RET) * CAP + ri % RET)).astype(F32).astype(BF)

    def enter(chunk):
        waited = arrived.at[pl.ds(0, 15)] if chunk == 0 else arrived.at[pl.ds(16, 16)]
        landed(waited, d_r.at[chunk])
        block = jnp.concatenate(
            [arrived[16 * chunk + i].astype(F32) for i in range(16)], axis=0
        ).astype(BF)
        tight = dot(squeeze, block).astype(BF)
        part = pl.ds(chunk * CHUNK, CHUNK)
        xr[part, own] = tight[:CHUNK]
        cr[part, own] = tight[CHUNK:]
        pair = []
        for n, (buf, u) in enumerate(((xr, "x"), (cr, "y"))):
            total = buf.at[part, pl.ds(0, 15 * LANES)]
            view = lane_blocks(buf, chunk * CHUNK, CHUNK)
            pair.append(PlaneGather(s, view, u, g_s.at[2 * chunk + n], g_r.at[2 * chunk + n], log, total))
        for g in pair:
            g.stage0()
        for g in pair:
            g.fan(0)
        gathers.append(pair)

    def gather(chunk, k):
        for g in gathers[chunk]:
            getattr(g, f"stage{k}")()

    def expert(chunk):
        if chunk == 0:
            for cp in loads:
                cp.wait()
        part = pl.ds(chunk * CHUNK, CHUNK)
        pre = dot(xr[part, :], wcat[...])
        pgate, up = pre[:, :LANES], pre[:, LANES:]
        sig = jax.nn.sigmoid(pgate)
        act = pgate * sig
        slope = sig * (1.0 + pgate * (1.0 - sig))
        hid[part, :] = (act * up).astype(BF)
        gh = dot_t(cr[part, :], wdv[...])
        grads = jnp.concatenate([(gh * up * slope).astype(BF), (gh * act).astype(BF)], axis=1)
        gp[part, :] = grads
        for far in (2, 1, 3, 0):
            for i in range(2):
                places = []
                for k in (2 * i, 2 * i + 1):
                    if chunk == 0:
                        places.append((k, s.col("x", far)))
                    else:
                        places.append((s.col("y", far), k))
                w2 = jnp.concatenate(
                    [wcat[pl.ds(pl.multiple_of((a * 4 + b) * LANES, LANES), LANES), :] for a, b in places],
                    axis=0,
                )
                t2 = dot_t(grads, w2).astype(BF)
                for n, (a, b) in enumerate(places):
                    terms[a, b, part, :] = t2[:, n * LANES : (n + 1) * LANES]
            if far == 2:
                sums[chunk].stage0()

    def summed(chunk, k):
        getattr(sums[chunk], f"stage{k}")()

    def leave(chunk):
        total = sums[chunk].stage4()
        ret[pl.ds(16 * chunk, 16)] = dot(spread, total).astype(BF).reshape(16, RET, LANES)
        to_all(lambda k: ret.at[k], lambda pos: back.at[2 * pos + s.c], r_s, r_r.at[chunk], origin, chunk)

    def rung(k):
        ring.step(k)

    enter(0)
    gather(0, 1)
    enter(1)
    rung(0)
    gather(0, 2)
    gather(0, 3)
    gather(1, 1)
    rung(1)
    gather(0, 4)
    gather(1, 2)
    gather(0, 5)
    gather(1, 3)
    rung(2)
    gather(0, 6)
    expert(0)
    gather(1, 4)
    rung(3)
    summed(0, 1)
    gather(1, 5)
    gather(1, 6)
    summed(0, 2)
    expert(1)
    rung(4)
    summed(0, 3)
    summed(1, 1)
    leave(0)
    rung(5)
    summed(1, 2)
    summed(1, 3)
    leave(1)
    back[pl.ds(s.c, 1)] = ret[pl.ds(s.c, 1)]
    rung(6)

    @pl.loop(0, 8)
    def _(i):
        lanes = pl.ds(pl.multiple_of(i * 2 * LANES, 2 * LANES), 2 * LANES)
        block = dot_0(xr[:, lanes], gp[...])
        gg_out[0, lanes, :] = block[:, :LANES]
        gu_out[0, lanes, :] = block[:, LANES:]
        gd_out[0, :, lanes] = dot_0(hid[...], cr[:, lanes])

    rung(7)
    send(opt.at[oprows, :], opt.at[oprows, :], h_s, h_r, sibling, log)
    lane = iota((LANES, 32 * RET), 1)
    spots = down[:, 0:2].astype(I32)
    want = ((lane == spots[:, 0:1]) | (lane == spots[:, 1:2])).astype(F32).astype(BF)
    landed(back.at[pl.ds(0, 15)], r_r.at[0])
    landed(back.at[pl.ds(16, 16)], r_r.at[1])
    grown = dot(want, back[...].reshape(32 * RET, LANES))
    tok = (cot32 + grown).astype(BF)
    toks[:, own] = tok

    inplace = s.z == s.tp
    odd = s.z % 2
    for q in range(8):
        col = 2 * q + odd
        src = toks.at[pl.ds(16 * q, 16), own]
        keep = jnp.logical_and(inplace, col == s.tp)

        @pl.when(jnp.logical_not(keep))
        def _():
            send(src, gt.at[s.z // 2, odd, q], x_s.at[q], x_r.at[s.z // 2], (2 * s.tp + s.c, col), [])

        @pl.when(keep)
        def _():
            gt[s.z // 2, odd, q] = src[...]

    fans = PlaneCast(s, lane_blocks(toks, 0, toks.shape[0]), t_s, t_r)
    fans.start()
    for i in range(8):
        keep = jnp.logical_and(inplace, s.z // 2 == i)

        @pl.when(jnp.logical_not(keep))
        def _():
            landed(gt.at[i, s.tp % 2, s.tp // 2], x_r.at[i])

    turns = PlaneCast(s, row_blocks(gt, 0, 8), u_s, u_r)
    turns.start()
    landed(opt.at[pl.ds(pl.multiple_of((1 - s.c) * halfw, 16), halfw), :], h_r)
    fans.finish()
    gm = dot_t(opt[...], toks[...])
    act_g, decays, states = act_v[...], dec_v[...], st_ref[...]
    local = gm * act_g
    for k in range(7):
        local = local + spans[k] * shifted_up(local, 2**k, 0.0)
    ent[s.sp] = turned(decays * local)[0:1]
    for chunk in (1, 0):
        to_all(lambda k: ent.at[s.sp], lambda pos: ent.at[s.sp], e_s, e_r, dest, chunk)
    ggb_out[...] = (gm * states * dact_v[...]).astype(BF)
    turns.finish()
    gops[...] = dot(mx[...], gt[...].reshape(16 * LANES, LANES))
    send(gops, gopr, z_s, z_r, sibling, log)

    landed(whole.at[pl.ds(0, 31)], w_r)
    landed(prevrow, l_r)
    prev = turned(jnp.broadcast_to(jnp.where(s.sp == 0, 0.0, prevrow[0]), (LANES, states.shape[0])))
    prev = jnp.where(iota(states.shape, 1) == 0, prev, pltpu.roll(states, 1, 1)) * decays
    landed(ent.at[pl.ds(0, 31)], e_r)
    carry = jnp.zeros((1, states.shape[0]), F32)
    for k in range(31, 0, -1):
        carry = jnp.where(s.sp < k, ent[k] + whole[k] * carry, carry)
    full = local + spans[7] * turned(jnp.broadcast_to(carry, (LANES, states.shape[0])))
    git_out[...] = full
    gld_out[...] = (full * prev).astype(BF)
    landed(gopr, z_r)
    gop = turned(gops[...] + gopr[...])
    gop_out[...] = jnp.where(first, gop[:64], gop[64:])

    for cp in log:
        cp.wait_send()
    for q in range(8):
        keep = jnp.logical_and(inplace, 2 * q + odd == s.tp)

        @pl.when(jnp.logical_not(keep))
        def _():
            landed(toks.at[pl.ds(16 * q, 16), own], x_s.at[q])

    fans.drain()
    turns.drain()
    for g in gathers[0] + gathers[1]:
        g.drain()
    landed(msg.at[pl.ds(0, 31)], d_s)
    landed(ret.at[pl.ds(0, 31)], r_s)
    landed(ent.at[pl.ds(0, 31)], e_s)
    landed(whole.at[pl.ds(0, 31)], w_s)


def settle(*refs):
    copies = [pltpu.make_async_copy(refs[k], refs[7 + k], refs[14].at[k]) for k in range(7)]
    for cp in copies:
        cp.start()
    for cp in copies:
        cp.wait()


def step(x, cot, routes, rw, gate, ld, st, wg, wu, wd, op):
    vm = pl.BlockSpec(memory_space=pltpu.VMEM)
    hb = pl.BlockSpec(memory_space=pltpu.MemorySpace.HBM)
    d = 16 * LANES
    w = gate.shape[1]
    V = pltpu.VMEM
    dma = pltpu.SemaphoreType.DMA
    S = jax.ShapeDtypeStruct
    sums = lambda: [
        V((4, HALF, LANES), BF), V((4, HALF, LANES), BF), V((4, CHUNK, LANES), BF), V((4, CHUNK, LANES), BF),
        V((4, CHUNK, LANES), BF),
        V((HALF, LANES), BF), V((HALF, LANES), BF), V((CHUNK, LANES), BF), V((CHUNK, LANES), BF),
    ]
    operands = (x, cot, routes.T, rw.T, gate.T, ld.T, st.T, op, wg, wu, wd)
    gg, gu, gd, gop, ggb, gld, git = pl.pallas_call(
        body,
        out_shape=[
            S(wg.shape, F32), S(wu.shape, F32), S(wd.shape, F32),
            S(op.shape, F32), S((w, LANES), BF), S((w, LANES), BF), S((w, LANES), F32),
        ],
        in_specs=[hb] * 11,
        out_specs=[vm] * 7,
        scratch_shapes=[
            V(x.shape, BF), V(cot.shape, BF), V((2, LANES), I32), V((2, LANES), F32),
            V((w, LANES), BF), V((w, LANES), F32), V((w, LANES), F32), V(op.shape, BF),
            V((32, MSG, LANES), BF), V((32, MSG, LANES), BF), V((ROWS, d), BF), V((ROWS, d), BF),
            V((d, 2 * LANES), BF), V((LANES, d), BF), V((ROWS, 2 * LANES), BF), V((ROWS, LANES), BF),
            V((4, 4, ROWS, LANES), BF), V((32, RET, LANES), BF), V((32, RET, LANES), BF),
            *sums(), *sums(),
            V(op.shape, BF), V((w, d), BF), V((w, d), BF), V((8, w, LANES), F32),
            V((w, LANES), F32), V((w, LANES), F32), V((w, LANES), F32),
            V((LANES, d), BF), V((8, 2, 8, 16, LANES), BF), V((32, 1, w), F32), V((32, 1, w), F32),
            V((1, 1, w), F32), V((1, 1, w), F32), V((w, LANES), F32), V((w, LANES), F32),
            dma((8,)), dma((3,)), dma, dma((2,)), dma((4,)), dma((4, 20)),
            dma((2, 8)), dma((2, 8)), dma, dma((2,)),
            dma, dma, dma((2, 2, 8)), dma((2, 2, 8)), dma((16,)), dma((16,)), dma((16,)), dma((16,)),
            dma((8,)), dma((8,)), dma, dma, dma, dma, dma, dma, dma, dma, dma, dma,
        ],
        compiler_params=pltpu.CompilerParams(
            collective_id=0, has_side_effects=True, vmem_limit_bytes=VMEM_MIB * 1024 * 1024
        ),
        name="whole_step",
    )(*[pltpu.with_memory_space_constraint(a, pltpu.MemorySpace.HBM) for a in operands])

    outs = (gg, gu, gd, gop, ggb, gld, git)
    gg, gu, gd, gop, ggb, gld, git = pl.pallas_call(
        settle,
        out_shape=[S(o.shape, o.dtype) for o in outs],
        in_specs=[vm] * 7,
        out_specs=[hb] * 7,
        scratch_shapes=[dma((7,))],
        compiler_params=pltpu.CompilerParams(vmem_limit_bytes=4 * 1024 * 1024),
        name="settle",
    )(*outs)
    return gg, gu, gd, gop, ggb.T, gld.T, git.T


def solution(mesh):
    both, rows = P("sp", "tp"), P("sp", None)
    last, middle = P("sp", None, "tp"), P("sp", "tp", None)
    return jax.shard_map(
        step,
        mesh=mesh,
        in_specs=(both, both, rows, rows, both, both, both, last, last, middle, both),
        out_specs=(last, last, middle, both, both, both, both),
        check_vma=False,
    )
```

```python
import functools

import jax
import jax.numpy as jnp
from jax import lax
from jax.experimental import pallas as pl
from jax.experimental.pallas import tpu as pltpu
from jax.sharding import PartitionSpec as P

BF = jnp.bfloat16
F32 = jnp.float32
I32 = jnp.int32
MESH = pl.DeviceIdType.MESH
LANES = 128
NZ = 16
CAP = 10
MSG = 24
RET = 16
ROWS = 2 * NZ * CAP
CHUNK = ROWS // 2
HALF = CHUNK // 2
VMEM_MIB = 30


def place(step):
    return max(2 * step - 1, 0) if step <= NZ // 2 else 2 * (NZ - step)


STEP_AT = [0] * NZ
for _step in range(NZ):
    STEP_AT[place(_step)] = _step


def dot(a, b):
    return jnp.dot(a, b, preferred_element_type=F32)


def dot_t(a, b):
    return lax.dot_general(a, b, (((1,), (1,)), ((), ())), preferred_element_type=F32)


def iota(shape, dim):
    return lax.broadcasted_iota(I32, shape, dim)


def landed(ref, sem):
    pltpu.make_async_copy(ref, ref, sem).wait()


class Spot:
    def __init__(self):
        self.sp = lax.axis_index("sp")
        self.tp = lax.axis_index("tp")
        self.z, self.c = self.sp // 2, self.sp % 2
        self.y, self.x = self.tp // 4, self.tp % 4

    def col(self, axis, by):
        return lax.rem(getattr(self, axis) + (by + 4), 4)

    def tpi(self, axis, by, other=0):
        a = self.col(axis, by)
        if axis == "x":
            return self.col("y", other) * 4 + a
        return a * 4 + self.col("x", other)

    def peer(self, axis, by):
        return (self.sp, self.tpi(axis, by))


def send(src, dst, ssem, rsem, dev, log):
    cp = pltpu.make_async_remote_copy(
        src_ref=src, dst_ref=dst, send_sem=ssem, recv_sem=rsem, device_id=dev, device_id_type=MESH
    )
    cp.start()
    log.append(cp)


class PlaneGather:
    def __init__(self, spot, view, u, ssem, rsem, buf, rows):
        self.s, self.block, self.u = spot, view, u
        self.v = "y" if u == "x" else "x"
        self.ssem, self.rsem, self.buf, self.rows = ssem, rsem, buf, rows
        self.fu = (0, -1, 1, 2)

    def view(self, du, dv, half=None):
        return self.block(self.s.tpi(self.u, du, dv), half)

    def go(self, view, axis, by, k):
        send(view, view, self.ssem, self.rsem.at[k], self.s.peer(axis, by), [])

    def fan(self, j):
        view = self.view(self.fu[j], 0)
        for by in (1, -1, 2):
            self.go(view, self.v, by, 3)

    def stage0(self):
        view = self.view(0, 0)
        for k, by in enumerate((1, -1, 2)):
            self.go(view, self.u, by, k)

    def stage1(self):
        for j in (1, 2):
            landed(self.view(self.fu[j], 0), self.rsem.at[j - 1])
            self.fan(j)

    def stage2(self):
        landed(self.view(2, 0), self.rsem.at[2])
        self.fan(3)

    def stage3(self):
        landed(self.buf.at[self.rows, pl.ds(0, 12 * LANES)], self.rsem.at[3])

    def drain(self):
        landed(self.buf.at[self.rows, pl.ds(0, 15 * LANES)], self.ssem)


class PlaneCast:
    def __init__(self, spot, view, ssem, rsem, total):
        self.s, self.view, self.ssem, self.rsem, self.total = spot, view, ssem, rsem, total
        self.moves = [(dy, dx) for dy in (2, 1, 3, 0) for dx in (2, 1, 3, 0) if dy or dx]

    def start(self):
        block = self.view(self.s.tp, None)
        for dy, dx in self.moves:
            dev = (self.s.sp, self.s.tpi("y", dy, dx))
            send(block, block, self.ssem, self.rsem, dev, [])

    def finish(self):
        landed(self.total, self.rsem)

    def drain(self):
        landed(self.total, self.ssem)


def lane_blocks(buf, r0, n):
    def view(tpi, half):
        lane = pl.ds(pl.multiple_of(tpi * LANES, LANES), LANES)
        if half is None:
            return buf.at[pl.ds(r0, n), lane]
        return buf.at[pl.ds(r0 + half * (n // 2), n // 2), lane]

    return view


def row_blocks(buf, i0, n):
    def view(tpi, half):
        if half is None:
            return buf.at[pl.ds(i0, n), tpi % 2, tpi // 2]
        return buf.at[pl.ds(i0 + half * (n // 2), n // 2), tpi % 2, tpi // 2]

    return view


class Ring:
    def __init__(self, spot, part, ssem, rsem):
        self.s, self.part, self.ssem, self.rsem = spot, part, ssem, rsem

    def at(self, by):
        return lax.rem(self.s.z + (by + NZ), NZ)

    def go(self, way, k):
        by = 1 if way == 0 else -1
        dev = (2 * self.at(by) + self.s.c, self.s.tp)
        view = self.part(self.at(-by * k))
        send(view, view, self.ssem, self.rsem.at[way, k], dev, [])

    def start(self):
        self.go(0, 0)
        self.go(1, 0)

    def step(self, k):
        for way, by, last in ((0, 1, 8), (1, -1, 7)):
            if k < last:
                landed(self.part(self.at(-by * (k + 1))), self.rsem.at[way, k])
                if k + 1 < last:
                    self.go(way, k + 1)


class PlaneSum:
    def __init__(self, spot, buf, r0, u, one, part, two, ssem, rsem):
        self.s, self.buf, self.r0, self.u = spot, buf, r0, u
        self.v = "y" if u == "x" else "x"
        self.one, self.part, self.two = one, part, two
        self.ssem, self.rsem = ssem, rsem

    def block(self, du):
        a = self.s.col(self.u, du)
        if self.u == "x":
            return self.buf.at[:, a, pl.ds(self.r0, HALF), :]
        return self.buf.at[a, :, pl.ds(self.r0, HALF), :]

    def go(self, src, dst, axis, by, k):
        send(src, dst, self.ssem, self.rsem.at[k], self.s.peer(axis, by), [])

    def stage0(self):
        for k, by in enumerate((2, 1, -1)):
            self.go(self.block(by), self.one.at[k], self.u, by, 0)

    def stage1(self):
        total = self.block(0)[...].astype(F32)
        landed(self.one, self.rsem.at[0])
        for k in range(3):
            total = total + self.one[k].astype(F32)
        self.part[...] = total.astype(BF)
        for k, by in enumerate((2, 1, -1)):
            self.go(self.part.at[self.s.col(self.v, by)], self.two.at[k], self.v, by, 1)

    def stage2(self):
        total = self.part[self.s.col(self.v, 0)].astype(F32)
        landed(self.two, self.rsem.at[1])
        for k in range(3):
            total = total + self.two[k].astype(F32)
        return total.astype(BF)


def dest(spot, step, core):
    return (2 * lax.rem(spot.z + (NZ - step), NZ) + core, spot.tp)


def origin(spot, step, core):
    return (2 * lax.rem(spot.z + step, NZ) + core, spot.tp)


def group_of(expert, z):
    step = lax.rem(z - expert // 2 + NZ, NZ)
    at = jnp.where(step <= NZ // 2, jnp.maximum(2 * step - 1, 0), 2 * (NZ - step))
    return at * 2 + expert % 2


def slots_by_lane(routes_t, z):
    tok = routes_t.shape[1]
    hot = [(iota((32, tok), 0) == routes_t[k : k + 1, :]) for k in range(2)]
    both = (hot[0] | hot[1]).astype(F32).astype(BF)
    earlier = (iota((tok, tok), 0) < iota((tok, tok), 1)).astype(F32).astype(BF)
    before = dot(both, earlier)
    slot = [jnp.sum(jnp.where(h, before, 0.0), axis=0, keepdims=True).astype(I32) for h in hot]
    return [(group_of(routes_t[k : k + 1, :], z), slot[k]) for k in range(2)]


def dot_0(a, b):
    return lax.dot_general(a, b, (((0,), (0,)), ((), ())), preferred_element_type=F32)


def shifted_up(v, by, fill):
    n = v.shape[1]
    return jnp.where(iota(v.shape, 1) < n - by, pltpu.roll(v, n - by, 1), fill)


def turned(v):
    if v.shape[1] == LANES:
        low = jnp.concatenate([v[LANES:], jnp.zeros((2 * LANES - v.shape[0], LANES), F32)], axis=0)
        return jnp.concatenate([v[:LANES].T, low.T[:, : v.shape[0] - LANES]], axis=1)
    wide = jnp.concatenate([v[:, LANES:], jnp.zeros((v.shape[0], 2 * LANES - v.shape[1]), F32)], axis=1)
    return jnp.concatenate([v[:, :LANES].T, wide.T[: v.shape[1] - LANES]], axis=0)


def body(
    x_in, cot_in, routes_in, rw_in, gate_in, ld_in, st_in, op_in, wg_ref, wu_ref, wd_ref,
    gg_out, gu_out, gd_out, gop_out, ggb_out, gld_out, git_out,
    x_ref, cot_ref, routes_t_ref, rw_t_ref, gate_ref, ld_ref, st_ref, op_ref,
    msg, arrived, xr, cr, wcat, wdv, gp, hid, terms, ret, back,
    one, part_v, two,
    opsib, mo, osib, spans, act_v, dact_v, dec_v, lead_v,
    toks, gt, ent, whole, lastrow, prevrow, gops, gopr,
    isem, wsem, d_s, d_r, g_s, g_r, q_s, q_r, r_s, r_r,
    o_s, o_r, ring_s, ring_r, t_s, t_r, u_s, u_r, x_s, x_r, e_s, e_r, w_s, w_r, l_s, l_r, h_s, h_r, z_s, z_r,
):
    inputs = [
        pltpu.make_async_copy(src, dst, isem.at[k])
        for k, (src, dst) in enumerate(
            (
                (routes_in, routes_t_ref), (rw_in, rw_t_ref), (x_in, x_ref), (cot_in, cot_ref),
                (op_in, op_ref), (gate_in, gate_ref), (st_in, st_ref), (ld_in, ld_ref),
            )
        )
    ]
    for cp in inputs:
        cp.start()
    s = Spot()
    log = []
    sibling = (2 * s.z + (1 - s.c), s.tp)
    barrier = pltpu.get_barrier_semaphore()
    peers = 1
    pl.semaphore_signal(barrier, inc=1, device_id=sibling, device_id_type=MESH)
    for step in range(1, NZ):
        for core in range(2):
            pl.semaphore_signal(barrier, inc=1, device_id=dest(s, step, core), device_id_type=MESH)
            peers += 1
    for axis in ("x", "y"):
        for by in (1, -1, 2):
            pl.semaphore_signal(barrier, inc=1, device_id=s.peer(axis, by), device_id_type=MESH)
            peers += 1

    loads = [
        pltpu.make_async_copy(wg_ref.at[0], wcat.at[:, pl.ds(0, LANES)], wsem.at[0]),
        pltpu.make_async_copy(wu_ref.at[0], wcat.at[:, pl.ds(LANES, LANES)], wsem.at[1]),
        pltpu.make_async_copy(wd_ref.at[0], wdv, wsem.at[2]),
    ]
    for cp in loads:
        cp.start()

    def to_all(src_of, dst, ssem, rsem, target, chunk):
        for pos in range(8) if chunk == 0 else range(15, 7, -1):
            step = STEP_AT[pos]
            for turn in range(2):
                core = (s.c, 1 - s.c)[turn]
                if step == 0:
                    if turn == 0:
                        continue
                    dev = sibling
                else:
                    dev = target(s, step, core)
                send(src_of(2 * pos + core), dst(pos), ssem, rsem, dev, [])

    for cp in inputs[:2]:
        cp.wait()
    by_lane = slots_by_lane(routes_t_ref[...], s.z)
    rows = [g * MSG + t for g, t in by_lane]
    across = jnp.concatenate(
        [(g * RET + t).astype(F32) for g, t in by_lane] + [rw_t_ref[...], jnp.zeros((4, LANES), F32)], axis=0
    )
    down = across.T
    at = iota((32 * MSG, LANES), 0)
    for cp in inputs[2:4]:
        cp.wait()
    cot32 = cot_ref[...].astype(F32)
    picks = jnp.concatenate(
        [
            ((at == rows[0]) | (at == rows[1])).astype(F32).astype(BF),
            (at == rows[0] + CAP).astype(F32).astype(BF),
            (at == rows[1] + CAP).astype(F32).astype(BF),
        ],
        axis=1,
    )
    stuff = jnp.concatenate(
        [x_ref[...]] + [(down[:, 2 + k : 3 + k] * cot32).astype(BF) for k in range(2)], axis=0
    )
    packed = dot(picks, stuff)
    for g in range(32):
        msg[g] = packed[g * MSG : (g + 1) * MSG, :].astype(BF)

    pl.semaphore_wait(barrier, peers)

    for chunk in range(2):
        to_all(lambda k: msg.at[k], lambda pos: arrived.at[2 * pos + s.c], d_s, d_r.at[chunk], dest, chunk)
    for cp in inputs[4:]:
        cp.wait()
    send(op_ref, opsib, o_s, o_r, sibling, log)
    arrived[pl.ds(s.c, 1)] = msg[pl.ds(s.c, 1)]

    width = gate_ref.shape[0]
    halfw = width // 2
    gate = gate_ref[...].astype(F32)
    states = st_ref[...]
    root = 0.7978845608028654
    th = jnp.tanh(root * (gate + 0.044715 * (gate * gate * gate)))
    act_g = 0.5 * gate * (1.0 + th)
    act_v[...] = act_g
    dact_v[...] = 0.5 * (1.0 + th) + 0.5 * gate * (1.0 - th * th) * (root * (1.0 + 3 * 0.044715 * (gate * gate)))
    lanes_z = pl.ds(pl.multiple_of(s.z * LANES, LANES), LANES)
    mo[pl.ds(0, width), lanes_z] = (act_g * states).astype(BF)
    landed(opsib, o_r)
    mine, other = op_ref[...].astype(F32), opsib[...].astype(F32)
    first = s.c == 0
    both = jnp.concatenate([jnp.where(first, mine, other), jnp.where(first, other, mine)], axis=0)
    both = turned(both)
    oprows = pl.ds(width, halfw)
    mo[oprows, lanes_z] = jnp.where(first, both[:halfw], both[halfw:]).astype(BF)

    def ring_part(z):
        return mo.at[:, pl.ds(pl.multiple_of(z * LANES, LANES), LANES)]

    ring = Ring(s, ring_part, ring_s, ring_r)
    ring.start()

    decays = jnp.exp(ld_ref[...])
    dec_v[...] = decays
    span = shifted_up(decays, 1, 1.0)
    for k in range(7):
        spans[k] = span
        span = span * shifted_up(span, 2**k, 1.0)
    spans[7] = span
    whole[s.sp] = turned(span * decays)[0:1]
    lead = decays
    for k in range(7):
        lead = lead * jnp.where(iota(lead.shape, 1) >= 2**k, pltpu.roll(lead, 2**k, 1), 1.0)
    lead_v[...] = lead
    lastrow[0] = turned(states)[LANES - 1 :]
    for chunk in range(2):
        to_all(lambda k: whole.at[s.sp], lambda pos: whole.at[s.sp], w_s, w_r, dest, chunk)
    send(lastrow, prevrow, l_s, l_r, (lax.rem(s.sp + 1, 32), s.tp), log)

    ri = iota((2 * CHUNK, 16 * MSG), 0)
    ci = iota((2 * CHUNK, 16 * MSG), 1)
    second = ri >= CHUNK
    rr = jnp.where(second, ri - CHUNK, ri)
    squeeze = (ci == (rr // CAP) * MSG + rr % CAP + jnp.where(second, CAP, 0)).astype(F32).astype(BF)

    own = pl.ds(pl.multiple_of(s.tp * LANES, LANES), LANES)
    gathers = []
    sums = [
        [
            PlaneSum(
                s, terms, chunk * CHUNK + n * HALF, u, one.at[chunk, n], part_v.at[chunk, n], two.at[chunk, n],
                q_s.at[chunk, n], q_r.at[chunk, n],
            )
            for n, u in enumerate(("x", "y"))
        ]
        for chunk in range(2)
    ]
    ri = iota((16 * RET, CHUNK), 0)
    ci = iota((16 * RET, CHUNK), 1)
    spread = ((ri % RET < CAP) & (ci == (ri // RET) * CAP + ri % RET)).astype(F32).astype(BF)

    def enter(chunk):
        waited = arrived.at[pl.ds(0, 15)] if chunk == 0 else arrived.at[pl.ds(16, 16)]
        landed(waited, d_r.at[chunk])
        block = jnp.concatenate(
            [arrived[16 * chunk + i].astype(F32) for i in range(16)], axis=0
        ).astype(BF)
        tight = dot(squeeze, block).astype(BF)
        part = pl.ds(chunk * CHUNK, CHUNK)
        xr[part, own] = tight[:CHUNK]
        cr[part, own] = tight[CHUNK:]
        pair = []
        for n, (buf, u) in enumerate(((xr, "x"), (cr, "y"))):
            view = lane_blocks(buf, chunk * CHUNK, CHUNK)
            pair.append(PlaneGather(s, view, u, g_s.at[2 * chunk + n], g_r.at[2 * chunk + n], buf, part))
        for g in pair:
            g.stage0()
        for g in pair:
            g.fan(0)
        gathers.append(pair)

    def gather(chunk, k):
        for g in gathers[chunk]:
            getattr(g, f"stage{k}")()

    def expert(chunk):
        if chunk == 0:
            for cp in loads:
                cp.wait()
        part = pl.ds(chunk * CHUNK, CHUNK)
        pre = dot(xr[part, :], wcat[...])
        pgate, up = pre[:, :LANES], pre[:, LANES:]
        sig = jax.nn.sigmoid(pgate)
        act = pgate * sig
        slope = sig * (1.0 + pgate * (1.0 - sig))
        hid[part, :] = (act * up).astype(BF)
        gh = dot_t(cr[part, :], wdv[...])
        grads = jnp.concatenate([(gh * up * slope).astype(BF), (gh * act).astype(BF)], axis=1)
        gp[part, :] = grads
        for i in range(8):
            t2 = dot_t(grads, wcat[pl.ds(2 * i * LANES, 2 * LANES), :]).astype(BF)
            terms[i // 2, 2 * (i % 2), part, :] = t2[:, :LANES]
            terms[i // 2, 2 * (i % 2) + 1, part, :] = t2[:, LANES:]
        for q in sums[chunk]:
            q.stage0()

    def summed(chunk):
        for q in sums[chunk]:
            q.stage1()

    def leave(chunk):
        total = jnp.concatenate([q.stage2() for q in sums[chunk]], axis=0)
        ret[pl.ds(16 * chunk, 16)] = dot(spread, total).astype(BF).reshape(16, RET, LANES)
        to_all(lambda k: ret.at[k], lambda pos: back.at[2 * pos + s.c], r_s, r_r.at[chunk], origin, chunk)

    def rung(k):
        ring.step(k)

    enter(0)
    gather(0, 1)
    gather(0, 2)
    enter(1)
    rung(0)
    gather(1, 1)
    gather(0, 3)
    rung(1)
    gather(1, 2)
    expert(0)
    gather(1, 3)
    rung(2)
    expert(1)
    summed(0)
    rung(3)
    summed(1)
    leave(0)
    rung(4)
    leave(1)
    back[pl.ds(s.c, 1)] = ret[pl.ds(s.c, 1)]
    rung(5)

    @pl.loop(0, 8)
    def _(i):
        lanes = pl.ds(pl.multiple_of(i * 2 * LANES, 2 * LANES), 2 * LANES)
        block = dot_0(xr[:, lanes], gp[...])
        gg_out[0, lanes, :] = block[:, :LANES]
        gu_out[0, lanes, :] = block[:, LANES:]
        gd_out[0, :, lanes] = dot_0(hid[...], cr[:, lanes])

    rung(6)
    lane = iota((LANES, 32 * RET), 1)
    spots = down[:, 0:2].astype(I32)
    want = ((lane == spots[:, 0:1]) | (lane == spots[:, 1:2])).astype(F32).astype(BF)
    landed(back.at[pl.ds(0, 15)], r_r.at[0])
    landed(back.at[pl.ds(16, 16)], r_r.at[1])
    grown = dot(want, back[...].reshape(32 * RET, LANES))
    tok = (cot32 + grown).astype(BF)
    toks[:, own] = tok

    fans = []
    for n, u in enumerate(("x", "y")):
        r0, cnt = n * (toks.shape[0] // 2), toks.shape[0] // 2
        fans.append(PlaneGather(s, lane_blocks(toks, r0, cnt), u, t_s.at[n], t_r.at[n], toks, pl.ds(r0, cnt)))
    for f in fans:
        f.stage0()
    for f in fans:
        f.fan(0)
    inplace = s.z == s.tp
    odd = s.z % 2
    for q in range(8):
        col = 2 * q + odd
        src = toks.at[pl.ds(16 * q, 16), own]
        keep = jnp.logical_and(inplace, col == s.tp)

        @pl.when(jnp.logical_not(keep))
        def _():
            send(src, gt.at[s.z // 2, odd, q], x_s, x_r, (2 * s.tp + s.c, col), [])

        @pl.when(keep)
        def _():
            gt[s.z // 2, odd, q] = src[...]

    def turned_in(sem):
        @pl.when(inplace)
        def _():
            landed(toks.at[pl.ds(0, 112), own], sem)

        @pl.when(jnp.logical_not(inplace))
        def _():
            landed(toks.at[pl.ds(0, 128), own], sem)

    rung(7)
    send(mo.at[oprows, :], osib, h_s, h_r, sibling, log)
    for k in (1, 2, 3):
        for f in fans:
            getattr(f, f"stage{k}")()
    landed(osib, h_r)
    halves = (dot_t(mo[oprows, :], toks[...]), dot_t(osib[...], toks[...]))
    gm = jnp.concatenate([jnp.where(first, halves[0], halves[1]), jnp.where(first, halves[1], halves[0])], axis=0)
    act_g, decays, states = act_v[...], dec_v[...], st_ref[...]
    local = gm * act_g
    ent[s.sp] = jnp.sum(turned(lead_v[...] * local), axis=0, keepdims=True)
    for chunk in (1, 0):
        to_all(lambda k: ent.at[s.sp], lambda pos: ent.at[s.sp], e_s, e_r, dest, chunk)
    turned_in(x_r)
    turns = PlaneCast(s, row_blocks(gt, 0, 8), u_s, u_r, toks.at[:, pl.ds(0, 15 * LANES)])
    turns.start()
    for k in range(7):
        local = local + spans[k] * shifted_up(local, 2**k, 0.0)
    ggb_out[...] = (gm * states * dact_v[...]).astype(BF)
    turns.finish()
    gops[...] = dot(mo[pl.ds(0, width), :], gt[...].reshape(16 * LANES, LANES))
    send(gops, gopr, z_s, z_r, sibling, log)

    landed(whole.at[pl.ds(0, 31)], w_r)
    landed(prevrow, l_r)
    prev = turned(jnp.broadcast_to(jnp.where(s.sp == 0, 0.0, prevrow[0]), (LANES, states.shape[0])))
    prev = jnp.where(iota(states.shape, 1) == 0, prev, pltpu.roll(states, 1, 1)) * decays
    landed(ent.at[pl.ds(0, 31)], e_r)
    carry = jnp.zeros((1, states.shape[0]), F32)
    for k in range(31, 0, -1):
        carry = jnp.where(s.sp < k, ent[k] + whole[k] * carry, carry)
    full = local + spans[7] * turned(jnp.broadcast_to(carry, (LANES, states.shape[0])))
    git_out[...] = full
    gld_out[...] = (full * prev).astype(BF)
    landed(gopr, z_r)
    gop = turned(gops[...] + gopr[...])
    gop_out[...] = jnp.where(first, gop[:64], gop[64:])

    for cp in log:
        cp.wait_send()
    turned_in(x_s)
    landed(mo.at[:, pl.ds(0, 15 * LANES)], ring_s)
    turns.drain()
    for g in gathers[0] + gathers[1] + fans:
        g.drain()
    for q in sums[0] + sums[1]:
        landed(xr.at[pl.ds(0, HALF), pl.ds(0, 15 * LANES)], q.ssem)
    landed(msg.at[pl.ds(0, 31)], d_s)
    landed(ret.at[pl.ds(0, 31)], r_s)
    landed(ent.at[pl.ds(0, 31)], e_s)
    landed(whole.at[pl.ds(0, 31)], w_s)


def settle(*refs):
    copies = [pltpu.make_async_copy(refs[k], refs[7 + k], refs[14].at[k]) for k in range(7)]
    for cp in copies:
        cp.start()
    for cp in copies:
        cp.wait()


def step(x, cot, routes, rw, gate, ld, st, wg, wu, wd, op):
    vm = pl.BlockSpec(memory_space=pltpu.VMEM)
    hb = pl.BlockSpec(memory_space=pltpu.MemorySpace.HBM)
    d = 16 * LANES
    w = gate.shape[1]
    V = pltpu.VMEM
    dma = pltpu.SemaphoreType.DMA
    S = jax.ShapeDtypeStruct
    operands = (x, cot, routes.T, rw.T, gate.T, ld.T, st.T, op, wg, wu, wd)
    gg, gu, gd, gop, ggb, gld, git = pl.pallas_call(
        body,
        out_shape=[
            S(wg.shape, F32), S(wu.shape, F32), S(wd.shape, F32),
            S(op.shape, F32), S((w, LANES), BF), S((w, LANES), BF), S((w, LANES), F32),
        ],
        in_specs=[hb] * 11,
        out_specs=[vm] * 7,
        scratch_shapes=[
            V(x.shape, BF), V(cot.shape, BF), V((2, LANES), I32), V((2, LANES), F32),
            V((w, LANES), BF), V((w, LANES), F32), V((w, LANES), F32), V(op.shape, BF),
            V((32, MSG, LANES), BF), V((32, MSG, LANES), BF), V((ROWS, d), BF), V((ROWS, d), BF),
            V((d, 2 * LANES), BF), V((LANES, d), BF), V((ROWS, 2 * LANES), BF), V((ROWS, LANES), BF),
            V((4, 4, ROWS, LANES), BF), V((32, RET, LANES), BF), V((32, RET, LANES), BF),
            V((2, 2, 3, 4, HALF, LANES), BF), V((2, 2, 4, HALF, LANES), BF), V((2, 2, 3, HALF, LANES), BF),
            V(op.shape, BF), V((w + w // 2, d), BF), V((w // 2, d), BF), V((8, w, LANES), F32),
            V((w, LANES), F32), V((w, LANES), F32), V((w, LANES), F32), V((w, LANES), F32),
            V((LANES, d), BF), V((8, 2, 8, 16, LANES), BF), V((32, 1, w), F32), V((32, 1, w), F32),
            V((1, 1, w), F32), V((1, 1, w), F32), V((w, LANES), F32), V((w, LANES), F32),
            dma((8,)), dma((3,)), dma, dma((2,)), dma((4,)), dma((4, 4)),
            dma((2, 2)), dma((2, 2, 2)), dma, dma((2,)),
            dma, dma, dma, dma((2, 8)), dma((2,)), dma((2, 4)), dma, dma,
            dma, dma, dma, dma, dma, dma, dma, dma, dma, dma, dma, dma,
        ],
        compiler_params=pltpu.CompilerParams(
            collective_id=0, has_side_effects=True, vmem_limit_bytes=VMEM_MIB * 1024 * 1024
        ),
        name="whole_step",
    )(*[pltpu.with_memory_space_constraint(a, pltpu.MemorySpace.HBM) for a in operands])

    outs = (gg, gu, gd, gop, ggb, gld, git)
    gg, gu, gd, gop, ggb, gld, git = pl.pallas_call(
        settle,
        out_shape=[S(o.shape, o.dtype) for o in outs],
        in_specs=[vm] * 7,
        out_specs=[hb] * 7,
        scratch_shapes=[dma((7,))],
        compiler_params=pltpu.CompilerParams(vmem_limit_bytes=4 * 1024 * 1024),
        name="settle",
    )(*outs)
    return gg, gu, gd, gop, ggb.T, gld.T, git.T


def solution(mesh):
    both, rows = P("sp", "tp"), P("sp", None)
    last, middle = P("sp", None, "tp"), P("sp", "tp", None)
    return jax.shard_map(
        step,
        mesh=mesh,
        in_specs=(both, both, rows, rows, both, both, both, last, last, middle, both),
        out_specs=(last, last, middle, both, both, both, both),
        check_vma=False,
    )
```

```python
import functools

import jax
import jax.numpy as jnp
from jax import lax
from jax.experimental import pallas as pl
from jax.experimental.pallas import tpu as pltpu
from jax.sharding import PartitionSpec as P

BF = jnp.bfloat16
F32 = jnp.float32
I32 = jnp.int32
MESH = pl.DeviceIdType.MESH
LANES = 128
NZ = 16
CAP = 10
MSG = 24
RET = 16
ROWS = 2 * NZ * CAP
CHUNK = ROWS // 2
HALF = CHUNK // 2
VMEM_MIB = 30


def place(step):
    return max(2 * step - 1, 0) if step <= NZ // 2 else 2 * (NZ - step)


STEP_AT = [0] * NZ
for _step in range(NZ):
    STEP_AT[place(_step)] = _step


def dot(a, b):
    return jnp.dot(a, b, preferred_element_type=F32)


def dot_t(a, b):
    return lax.dot_general(a, b, (((1,), (1,)), ((), ())), preferred_element_type=F32)


def iota(shape, dim):
    return lax.broadcasted_iota(I32, shape, dim)


def landed(ref, sem):
    pltpu.make_async_copy(ref, ref, sem).wait()


class Spot:
    def __init__(self):
        self.sp = lax.axis_index("sp")
        self.tp = lax.axis_index("tp")
        self.z, self.c = self.sp // 2, self.sp % 2
        self.y, self.x = self.tp // 4, self.tp % 4

    def col(self, axis, by):
        return lax.rem(getattr(self, axis) + (by + 4), 4)

    def tpi(self, axis, by, other=0):
        a = self.col(axis, by)
        if axis == "x":
            return self.col("y", other) * 4 + a
        return a * 4 + self.col("x", other)

    def peer(self, axis, by):
        return (self.sp, self.tpi(axis, by))


def send(src, dst, ssem, rsem, dev, log):
    cp = pltpu.make_async_remote_copy(
        src_ref=src, dst_ref=dst, send_sem=ssem, recv_sem=rsem, device_id=dev, device_id_type=MESH
    )
    cp.start()
    log.append(cp)


class PlaneGather:
    def __init__(self, spot, view, u, ssem, rsem, buf, rows):
        self.s, self.block, self.u = spot, view, u
        self.v = "y" if u == "x" else "x"
        self.ssem, self.rsem, self.buf, self.rows = ssem, rsem, buf, rows
        self.fu = (0, -1, 1, 2)

    def view(self, du, dv, half=None):
        return self.block(self.s.tpi(self.u, du, dv), half)

    def go(self, view, axis, by, k):
        send(view, view, self.ssem, self.rsem.at[k], self.s.peer(axis, by), [])

    def fan(self, j):
        view = self.view(self.fu[j], 0)
        for by in (1, -1, 2):
            self.go(view, self.v, by, 3)

    def stage0(self):
        view = self.view(0, 0)
        for k, by in enumerate((1, -1, 2)):
            self.go(view, self.u, by, k)

    def stage1(self):
        for j in (1, 2):
            landed(self.view(self.fu[j], 0), self.rsem.at[j - 1])
            self.fan(j)

    def stage2(self):
        landed(self.view(2, 0), self.rsem.at[2])
        self.fan(3)

    def stage3(self):
        landed(self.buf.at[self.rows, pl.ds(0, 12 * LANES)], self.rsem.at[3])

    def drain(self):
        landed(self.buf.at[self.rows, pl.ds(0, 15 * LANES)], self.ssem)


class RelayGather(PlaneGather):
    def fan(self, j):
        view = self.view(self.fu[j], 0)
        self.go(view, self.v, 1, 3 + 2 * j)
        self.go(view, self.v, -1, 4 + 2 * j)

    def stage0(self):
        view = self.view(0, 0)
        self.go(view, self.u, 1, 0)
        self.go(view, self.u, -1, 1)

    def pass_on(self, du, dv, axis, k, far):
        for n, by in enumerate((1, -1)):
            at = (-by, 0) if axis == self.u else (du, -by)
            landed(self.view(*at), self.rsem.at[k + n])
            self.go(self.view(*at, n), axis, by, far)
            if axis == self.u:
                self.fan(1 + n)

    def stage1(self):
        self.pass_on(0, 0, self.u, 0, 2)

    def stage2(self):
        landed(self.view(2, 0), self.rsem.at[2])
        self.fan(3)

    def stage3(self):
        self.pass_on(0, 0, self.v, 3, 11)

    def stage4(self):
        self.pass_on(-1, 0, self.v, 5, 11)
        self.pass_on(1, 0, self.v, 7, 11)

    def stage5(self):
        self.pass_on(2, 0, self.v, 9, 11)

    def stage6(self):
        landed(self.buf.at[self.rows, pl.ds(0, 4 * LANES)], self.rsem.at[11])


class PlaneCast:
    def __init__(self, spot, view, ssem, rsem, total):
        self.s, self.view, self.ssem, self.rsem, self.total = spot, view, ssem, rsem, total
        self.moves = [(dy, dx) for dy in (2, 1, 3, 0) for dx in (2, 1, 3, 0) if dy or dx]

    def start(self):
        block = self.view(self.s.tp, None)
        for dy, dx in self.moves:
            dev = (self.s.sp, self.s.tpi("y", dy, dx))
            send(block, block, self.ssem, self.rsem, dev, [])

    def finish(self):
        landed(self.total, self.rsem)

    def drain(self):
        landed(self.total, self.ssem)


def lane_blocks(buf, r0, n):
    def view(tpi, half):
        lane = pl.ds(pl.multiple_of(tpi * LANES, LANES), LANES)
        if half is None:
            return buf.at[pl.ds(r0, n), lane]
        return buf.at[pl.ds(r0 + half * (n // 2), n // 2), lane]

    return view


def row_blocks(buf, i0, n):
    def view(tpi, half):
        if half is None:
            return buf.at[pl.ds(i0, n), tpi % 2, tpi // 2]
        return buf.at[pl.ds(i0 + half * (n // 2), n // 2), tpi % 2, tpi // 2]

    return view


class Ring:
    def __init__(self, spot, part, ssem, rsem):
        self.s, self.part, self.ssem, self.rsem = spot, part, ssem, rsem

    def at(self, by):
        return lax.rem(self.s.z + (by + NZ), NZ)

    def go(self, way, k):
        by = 1 if way == 0 else -1
        dev = (2 * self.at(by) + self.s.c, self.s.tp)
        view = self.part(self.at(-by * k))
        send(view, view, self.ssem, self.rsem.at[way, k], dev, [])

    def start(self):
        self.go(0, 0)
        self.go(1, 0)

    def step(self, k):
        for way, by, last in ((0, 1, 8), (1, -1, 7)):
            if k < last:
                landed(self.part(self.at(-by * (k + 1))), self.rsem.at[way, k])
                if k + 1 < last:
                    self.go(way, k + 1)


class PlaneSum:
    def __init__(self, spot, buf, r0, u, one, part, two, ssem, rsem):
        self.s, self.buf, self.r0, self.u = spot, buf, r0, u
        self.v = "y" if u == "x" else "x"
        self.one, self.part, self.two = one, part, two
        self.ssem, self.rsem = ssem, rsem

    def block(self, du):
        a = self.s.col(self.u, du)
        if self.u == "x":
            return self.buf.at[:, a, pl.ds(self.r0, HALF), :]
        return self.buf.at[a, :, pl.ds(self.r0, HALF), :]

    def go(self, src, dst, axis, by, k):
        send(src, dst, self.ssem, self.rsem.at[k], self.s.peer(axis, by), [])

    def stage0(self):
        for k, by in enumerate((2, 1, -1)):
            self.go(self.block(by), self.one.at[k], self.u, by, 0)

    def stage1(self):
        total = self.block(0)[...].astype(F32)
        landed(self.one, self.rsem.at[0])
        for k in range(3):
            total = total + self.one[k].astype(F32)
        self.part[...] = total.astype(BF)
        for k, by in enumerate((2, 1, -1)):
            self.go(self.part.at[self.s.col(self.v, by)], self.two.at[k], self.v, by, 1)

    def stage2(self):
        total = self.part[self.s.col(self.v, 0)].astype(F32)
        landed(self.two, self.rsem.at[1])
        for k in range(3):
            total = total + self.two[k].astype(F32)
        return total.astype(BF)


def dest(spot, step, core):
    return (2 * lax.rem(spot.z + (NZ - step), NZ) + core, spot.tp)


def origin(spot, step, core):
    return (2 * lax.rem(spot.z + step, NZ) + core, spot.tp)


def group_of(expert, z):
    step = lax.rem(z - expert // 2 + NZ, NZ)
    at = jnp.where(step <= NZ // 2, jnp.maximum(2 * step - 1, 0), 2 * (NZ - step))
    return at * 2 + expert % 2


def slots_by_lane(routes_t, z):
    tok = routes_t.shape[1]
    hot = [(iota((32, tok), 0) == routes_t[k : k + 1, :]) for k in range(2)]
    both = (hot[0] | hot[1]).astype(F32).astype(BF)
    earlier = (iota((tok, tok), 0) < iota((tok, tok), 1)).astype(F32).astype(BF)
    before = dot(both, earlier)
    slot = [jnp.sum(jnp.where(h, before, 0.0), axis=0, keepdims=True).astype(I32) for h in hot]
    return [(group_of(routes_t[k : k + 1, :], z), slot[k]) for k in range(2)]


def dot_0(a, b):
    return lax.dot_general(a, b, (((0,), (0,)), ((), ())), preferred_element_type=F32)


def shifted_up(v, by, fill):
    n = v.shape[1]
    return jnp.where(iota(v.shape, 1) < n - by, pltpu.roll(v, n - by, 1), fill)


def turned(v):
    if v.shape[1] == LANES:
        low = jnp.concatenate([v[LANES:], jnp.zeros((2 * LANES - v.shape[0], LANES), F32)], axis=0)
        return jnp.concatenate([v[:LANES].T, low.T[:, : v.shape[0] - LANES]], axis=1)
    wide = jnp.concatenate([v[:, LANES:], jnp.zeros((v.shape[0], 2 * LANES - v.shape[1]), F32)], axis=1)
    return jnp.concatenate([v[:, :LANES].T, wide.T[: v.shape[1] - LANES]], axis=0)


def body(
    x_in, cot_in, routes_in, rw_in, gate_in, ld_in, st_in, op_in, wg_ref, wu_ref, wd_ref,
    gg_out, gu_out, gd_out, gop_out, ggb_out, gld_out, git_out,
    x_ref, cot_ref, routes_t_ref, rw_t_ref, gate_ref, ld_ref, st_ref, op_ref,
    msg, arrived, xr, cr, wcat, wdv, gp, hid, terms, ret, back,
    one, part_v, two,
    opsib, mo, osib, spans, act_v, dact_v, dec_v, lead_v,
    toks, gt, ent, whole, lastrow, prevrow, gops, gopr,
    isem, wsem, d_s, d_r, g_s, g_r, q_s, q_r, r_s, r_r,
    o_s, o_r, ring_s, ring_r, t_s, t_r, u_s, u_r, x_s, x_r, e_s, e_r, w_s, w_r, l_s, l_r, h_s, h_r, z_s, z_r,
):
    inputs = [
        pltpu.make_async_copy(src, dst, isem.at[k])
        for k, (src, dst) in enumerate(
            (
                (routes_in, routes_t_ref), (rw_in, rw_t_ref), (x_in, x_ref), (cot_in, cot_ref),
                (op_in, op_ref), (gate_in, gate_ref), (st_in, st_ref), (ld_in, ld_ref),
            )
        )
    ]
    for cp in inputs:
        cp.start()
    s = Spot()
    log = []
    sibling = (2 * s.z + (1 - s.c), s.tp)
    barrier = pltpu.get_barrier_semaphore()
    peers = 1
    pl.semaphore_signal(barrier, inc=1, device_id=sibling, device_id_type=MESH)
    for step in STEP_AT[:0:-1]:
        for core in range(2):
            pl.semaphore_signal(barrier, inc=1, device_id=dest(s, step, core), device_id_type=MESH)
            peers += 1
    for axis in ("x", "y"):
        for by in (1, -1, 2):
            pl.semaphore_signal(barrier, inc=1, device_id=s.peer(axis, by), device_id_type=MESH)
            peers += 1

    loads = [
        pltpu.make_async_copy(wg_ref.at[0], wcat.at[:, pl.ds(0, LANES)], wsem.at[0]),
        pltpu.make_async_copy(wu_ref.at[0], wcat.at[:, pl.ds(LANES, LANES)], wsem.at[1]),
        pltpu.make_async_copy(wd_ref.at[0], wdv, wsem.at[2]),
    ]
    for cp in loads:
        cp.start()

    def to_all(src_of, dst, ssem, rsem, target, chunk):
        for pos in range(8) if chunk == 0 else range(15, 7, -1):
            step = STEP_AT[pos]
            for turn in range(2):
                core = (s.c, 1 - s.c)[turn]
                if step == 0:
                    if turn == 0:
                        continue
                    dev = sibling
                else:
                    dev = target(s, step, core)
                send(src_of(2 * pos + core), dst(pos), ssem, rsem, dev, [])

    for cp in inputs[:2]:
        cp.wait()
    by_lane = slots_by_lane(routes_t_ref[...], s.z)
    rows = [g * MSG + t for g, t in by_lane]
    across = jnp.concatenate(
        [(g * RET + t).astype(F32) for g, t in by_lane] + [rw_t_ref[...], jnp.zeros((4, LANES), F32)], axis=0
    )
    down = across.T
    at = iota((32 * MSG, LANES), 0)
    for cp in inputs[2:4]:
        cp.wait()
    cot32 = cot_ref[...].astype(F32)
    picks = jnp.concatenate(
        [
            ((at == rows[0]) | (at == rows[1])).astype(F32).astype(BF),
            (at == rows[0] + CAP).astype(F32).astype(BF),
            (at == rows[1] + CAP).astype(F32).astype(BF),
        ],
        axis=1,
    )
    stuff = jnp.concatenate(
        [x_ref[...]] + [(down[:, 2 + k : 3 + k] * cot32).astype(BF) for k in range(2)], axis=0
    )
    packed = dot(picks, stuff)
    for g in range(32):
        msg[g] = packed[g * MSG : (g + 1) * MSG, :].astype(BF)

    pl.semaphore_wait(barrier, peers)

    for chunk in range(2):
        to_all(lambda k: msg.at[k], lambda pos: arrived.at[2 * pos + s.c], d_s, d_r.at[chunk], dest, chunk)
    for cp in inputs[4:]:
        cp.wait()
    send(op_ref, opsib, o_s, o_r, sibling, log)
    arrived[pl.ds(s.c, 1)] = msg[pl.ds(s.c, 1)]

    width = gate_ref.shape[0]
    halfw = width // 2
    gate = gate_ref[...].astype(F32)
    states = st_ref[...]
    root = 0.7978845608028654
    th = jnp.tanh(root * (gate + 0.044715 * (gate * gate * gate)))
    act_g = 0.5 * gate * (1.0 + th)
    act_v[...] = act_g
    dact_v[...] = 0.5 * (1.0 + th) + 0.5 * gate * (1.0 - th * th) * (root * (1.0 + 3 * 0.044715 * (gate * gate)))
    lanes_z = pl.ds(pl.multiple_of(s.z * LANES, LANES), LANES)
    mo[pl.ds(0, width), lanes_z] = (act_g * states).astype(BF)
    landed(opsib, o_r)
    mine, other = op_ref[...].astype(F32), opsib[...].astype(F32)
    first = s.c == 0
    both = jnp.concatenate([jnp.where(first, mine, other), jnp.where(first, other, mine)], axis=0)
    both = turned(both)
    oprows = pl.ds(width, halfw)
    mo[oprows, lanes_z] = jnp.where(first, both[:halfw], both[halfw:]).astype(BF)

    def ring_part(z):
        return mo.at[:, pl.ds(pl.multiple_of(z * LANES, LANES), LANES)]

    ring = Ring(s, ring_part, ring_s, ring_r)
    ring.start()

    decays = jnp.exp(ld_ref[...])
    dec_v[...] = decays
    span = shifted_up(decays, 1, 1.0)
    for k in range(7):
        spans[k] = span
        span = span * shifted_up(span, 2**k, 1.0)
    spans[7] = span
    whole[s.sp] = turned(span * decays)[0:1]
    lead = decays
    for k in range(7):
        lead = lead * jnp.where(iota(lead.shape, 1) >= 2**k, pltpu.roll(lead, 2**k, 1), 1.0)
    lead_v[...] = lead
    lastrow[0] = turned(states)[LANES - 1 :]

    ri = iota((2 * CHUNK, 16 * MSG), 0)
    ci = iota((2 * CHUNK, 16 * MSG), 1)
    second = ri >= CHUNK
    rr = jnp.where(second, ri - CHUNK, ri)
    squeeze = (ci == (rr // CAP) * MSG + rr % CAP + jnp.where(second, CAP, 0)).astype(F32).astype(BF)

    own = pl.ds(pl.multiple_of(s.tp * LANES, LANES), LANES)
    gathers = []
    sums = [
        [
            PlaneSum(
                s, terms, chunk * CHUNK + n * HALF, u, one.at[chunk, n], part_v.at[chunk, n], two.at[chunk, n],
                q_s.at[chunk, n], q_r.at[chunk, n],
            )
            for n, u in enumerate(("x", "y"))
        ]
        for chunk in range(2)
    ]
    ri = iota((16 * RET, CHUNK), 0)
    ci = iota((16 * RET, CHUNK), 1)
    spread = ((ri % RET < CAP) & (ci == (ri // RET) * CAP + ri % RET)).astype(F32).astype(BF)

    def enter(chunk):
        waited = arrived.at[pl.ds(0, 15)] if chunk == 0 else arrived.at[pl.ds(16, 16)]
        landed(waited, d_r.at[chunk])
        block = jnp.concatenate(
            [arrived[16 * chunk + i].astype(F32) for i in range(16)], axis=0
        ).astype(BF)
        tight = dot(squeeze, block).astype(BF)
        part = pl.ds(chunk * CHUNK, CHUNK)
        xr[part, own] = tight[:CHUNK]
        cr[part, own] = tight[CHUNK:]
        pair = []
        for n, (buf, u) in enumerate(((xr, "x"), (cr, "y"))):
            view = lane_blocks(buf, chunk * CHUNK, CHUNK)
            kind = RelayGather if chunk == 0 else PlaneGather
            pair.append(kind(s, view, u, g_s.at[2 * chunk + n], g_r.at[2 * chunk + n], buf, part))
        for g in pair:
            g.stage0()
        for g in pair:
            g.fan(0)
        gathers.append(pair)

    def gather(chunk, k):
        for g in gathers[chunk]:
            getattr(g, f"stage{k}")()

    def expert(chunk):
        if chunk == 0:
            for cp in loads:
                cp.wait()
        part = pl.ds(chunk * CHUNK, CHUNK)
        pre = dot(xr[part, :], wcat[...])
        pgate, up = pre[:, :LANES], pre[:, LANES:]
        sig = jax.nn.sigmoid(pgate)
        act = pgate * sig
        slope = sig * (1.0 + pgate * (1.0 - sig))
        hid[part, :] = (act * up).astype(BF)
        gh = dot_t(cr[part, :], wdv[...])
        grads = jnp.concatenate([(gh * up * slope).astype(BF), (gh * act).astype(BF)], axis=1)
        gp[part, :] = grads
        for i in range(8):
            t2 = dot_t(grads, wcat[pl.ds(2 * i * LANES, 2 * LANES), :]).astype(BF)
            terms[i // 2, 2 * (i % 2), part, :] = t2[:, :LANES]
            terms[i // 2, 2 * (i % 2) + 1, part, :] = t2[:, LANES:]
        for q in sums[chunk]:
            q.stage0()

    def summed(chunk):
        for q in sums[chunk]:
            q.stage1()

    def leave(chunk):
        total = jnp.concatenate([q.stage2() for q in sums[chunk]], axis=0)
        ret[pl.ds(16 * chunk, 16)] = dot(spread, total).astype(BF).reshape(16, RET, LANES)
        to_all(lambda k: ret.at[k], lambda pos: back.at[2 * pos + s.c], r_s, r_r.at[chunk], origin, chunk)

    def rung(k):
        ring.step(k)

    enter(0)
    gather(0, 1)
    rung(0)
    enter(1)
    gather(0, 2)
    gather(0, 3)
    rung(1)
    for chunk in range(2):
        to_all(lambda k: whole.at[s.sp], lambda pos: whole.at[s.sp], w_s, w_r, dest, chunk)
    send(lastrow, prevrow, l_s, l_r, (lax.rem(s.sp + 1, 32), s.tp), log)
    gather(0, 4)
    gather(1, 1)
    rung(2)
    gather(0, 5)
    gather(1, 2)
    rung(3)
    gather(0, 6)
    rung(4)
    expert(0)
    gather(1, 3)
    expert(1)
    rung(5)
    summed(0)
    summed(1)
    rung(6)
    leave(0)
    leave(1)
    rung(7)
    send(mo.at[oprows, :], osib, h_s, h_r, sibling, log)
    back[pl.ds(s.c, 1)] = ret[pl.ds(s.c, 1)]

    @pl.loop(0, 8)
    def _(i):
        lanes = pl.ds(pl.multiple_of(i * 2 * LANES, 2 * LANES), 2 * LANES)
        block = dot_0(xr[:, lanes], gp[...])
        gg_out[0, lanes, :] = block[:, :LANES]
        gu_out[0, lanes, :] = block[:, LANES:]
        gd_out[0, :, lanes] = dot_0(hid[...], cr[:, lanes])

    lane = iota((LANES, 32 * RET), 1)
    spots = down[:, 0:2].astype(I32)
    want = ((lane == spots[:, 0:1]) | (lane == spots[:, 1:2])).astype(F32).astype(BF)
    landed(back.at[pl.ds(0, 15)], r_r.at[0])
    landed(back.at[pl.ds(16, 16)], r_r.at[1])
    grown = dot(want, back[...].reshape(32 * RET, LANES))
    tok = (cot32 + grown).astype(BF)
    toks[:, own] = tok

    fans = []
    for n, u in enumerate(("x", "y")):
        r0, cnt = n * (toks.shape[0] // 2), toks.shape[0] // 2
        fans.append(PlaneGather(s, lane_blocks(toks, r0, cnt), u, t_s.at[n], t_r.at[n], toks, pl.ds(r0, cnt)))
    for f in fans:
        f.stage0()
    for f in fans:
        f.fan(0)
    inplace = s.z == s.tp
    odd = s.z % 2
    for q in range(8):
        col = 2 * q + odd
        src = toks.at[pl.ds(16 * q, 16), own]
        keep = jnp.logical_and(inplace, col == s.tp)

        @pl.when(jnp.logical_not(keep))
        def _():
            send(src, gt.at[s.z // 2, odd, q], x_s, x_r, (2 * s.tp + s.c, col), [])

        @pl.when(keep)
        def _():
            gt[s.z // 2, odd, q] = src[...]

    def turned_in(sem):
        @pl.when(inplace)
        def _():
            landed(toks.at[pl.ds(0, 112), own], sem)

        @pl.when(jnp.logical_not(inplace))
        def _():
            landed(toks.at[pl.ds(0, 128), own], sem)

    for k in (1, 2, 3):
        for f in fans:
            getattr(f, f"stage{k}")()
    landed(osib, h_r)
    halves = (dot_t(mo[oprows, :], toks[...]), dot_t(osib[...], toks[...]))
    gm = jnp.concatenate([jnp.where(first, halves[0], halves[1]), jnp.where(first, halves[1], halves[0])], axis=0)
    act_g, decays, states = act_v[...], dec_v[...], st_ref[...]
    local = gm * act_g
    ent[s.sp] = jnp.sum(turned(lead_v[...] * local), axis=0, keepdims=True)
    for chunk in (1, 0):
        to_all(lambda k: ent.at[s.sp], lambda pos: ent.at[s.sp], e_s, e_r, dest, chunk)
    turned_in(x_r)
    turns = PlaneCast(s, row_blocks(gt, 0, 8), u_s, u_r, toks.at[:, pl.ds(0, 15 * LANES)])
    turns.start()
    for k in range(7):
        local = local + spans[k] * shifted_up(local, 2**k, 0.0)
    ggb_out[...] = (gm * states * dact_v[...]).astype(BF)
    turns.finish()
    gops[...] = dot(mo[pl.ds(0, width), :], gt[...].reshape(16 * LANES, LANES))
    send(gops, gopr, z_s, z_r, sibling, log)

    landed(whole.at[pl.ds(0, 31)], w_r)
    landed(prevrow, l_r)
    prev = turned(jnp.broadcast_to(jnp.where(s.sp == 0, 0.0, prevrow[0]), (LANES, states.shape[0])))
    prev = jnp.where(iota(states.shape, 1) == 0, prev, pltpu.roll(states, 1, 1)) * decays
    landed(ent.at[pl.ds(0, 31)], e_r)
    carry = jnp.zeros((1, states.shape[0]), F32)
    for k in range(31, 0, -1):
        carry = jnp.where(s.sp < k, ent[k] + whole[k] * carry, carry)
    full = local + spans[7] * turned(jnp.broadcast_to(carry, (LANES, states.shape[0])))
    git_out[...] = full
    gld_out[...] = (full * prev).astype(BF)
    landed(gopr, z_r)
    gop = turned(gops[...] + gopr[...])
    gop_out[...] = jnp.where(first, gop[:64], gop[64:])

    for cp in log:
        cp.wait_send()
    turned_in(x_s)
    landed(mo.at[:, pl.ds(0, 15 * LANES)], ring_s)
    turns.drain()
    for g in gathers[0] + gathers[1] + fans:
        g.drain()
    for q in sums[0] + sums[1]:
        landed(xr.at[pl.ds(0, HALF), pl.ds(0, 15 * LANES)], q.ssem)
    landed(msg.at[pl.ds(0, 31)], d_s)
    landed(ret.at[pl.ds(0, 31)], r_s)
    landed(ent.at[pl.ds(0, 31)], e_s)
    landed(whole.at[pl.ds(0, 31)], w_s)


def settle(*refs):
    copies = [pltpu.make_async_copy(refs[k], refs[7 + k], refs[14].at[k]) for k in range(7)]
    for cp in copies:
        cp.start()
    for cp in copies:
        cp.wait()


def step(x, cot, routes, rw, gate, ld, st, wg, wu, wd, op):
    vm = pl.BlockSpec(memory_space=pltpu.VMEM)
    hb = pl.BlockSpec(memory_space=pltpu.MemorySpace.HBM)
    d = 16 * LANES
    w = gate.shape[1]
    V = pltpu.VMEM
    dma = pltpu.SemaphoreType.DMA
    S = jax.ShapeDtypeStruct
    operands = (x, cot, routes.T, rw.T, gate.T, ld.T, st.T, op, wg, wu, wd)
    gg, gu, gd, gop, ggb, gld, git = pl.pallas_call(
        body,
        out_shape=[
            S(wg.shape, F32), S(wu.shape, F32), S(wd.shape, F32),
            S(op.shape, F32), S((w, LANES), BF), S((w, LANES), BF), S((w, LANES), F32),
        ],
        in_specs=[hb] * 11,
        out_specs=[vm] * 7,
        scratch_shapes=[
            V(x.shape, BF), V(cot.shape, BF), V((2, LANES), I32), V((2, LANES), F32),
            V((w, LANES), BF), V((w, LANES), F32), V((w, LANES), F32), V(op.shape, BF),
            V((32, MSG, LANES), BF), V((32, MSG, LANES), BF), V((ROWS, d), BF), V((ROWS, d), BF),
            V((d, 2 * LANES), BF), V((LANES, d), BF), V((ROWS, 2 * LANES), BF), V((ROWS, LANES), BF),
            V((4, 4, ROWS, LANES), BF), V((32, RET, LANES), BF), V((32, RET, LANES), BF),
            V((2, 2, 3, 4, HALF, LANES), BF), V((2, 2, 4, HALF, LANES), BF), V((2, 2, 3, HALF, LANES), BF),
            V(op.shape, BF), V((w + w // 2, d), BF), V((w // 2, d), BF), V((8, w, LANES), F32),
            V((w, LANES), F32), V((w, LANES), F32), V((w, LANES), F32), V((w, LANES), F32),
            V((LANES, d), BF), V((8, 2, 8, 16, LANES), BF), V((32, 1, w), F32), V((32, 1, w), F32),
            V((1, 1, w), F32), V((1, 1, w), F32), V((w, LANES), F32), V((w, LANES), F32),
            dma((8,)), dma((3,)), dma, dma((2,)), dma((4,)), dma((4, 12)),
            dma((2, 2)), dma((2, 2, 2)), dma, dma((2,)),
            dma, dma, dma, dma((2, 8)), dma((2,)), dma((2, 4)), dma, dma,
            dma, dma, dma, dma, dma, dma, dma, dma, dma, dma, dma, dma,
        ],
        compiler_params=pltpu.CompilerParams(
            collective_id=0, has_side_effects=True, vmem_limit_bytes=VMEM_MIB * 1024 * 1024
        ),
        name="whole_step",
    )(*[pltpu.with_memory_space_constraint(a, pltpu.MemorySpace.HBM) for a in operands])

    outs = (gg, gu, gd, gop, ggb, gld, git)
    gg, gu, gd, gop, ggb, gld, git = pl.pallas_call(
        settle,
        out_shape=[S(o.shape, o.dtype) for o in outs],
        in_specs=[vm] * 7,
        out_specs=[hb] * 7,
        scratch_shapes=[dma((7,))],
        compiler_params=pltpu.CompilerParams(vmem_limit_bytes=4 * 1024 * 1024),
        name="settle",
    )(*outs)
    return gg, gu, gd, gop, ggb.T, gld.T, git.T


def solution(mesh):
    both, rows = P("sp", "tp"), P("sp", None)
    last, middle = P("sp", None, "tp"), P("sp", "tp", None)
    return jax.shard_map(
        step,
        mesh=mesh,
        in_specs=(both, both, rows, rows, both, both, both, last, last, middle, both),
        out_specs=(last, last, middle, both, both, both, both),
        check_vma=False,
    )
```
